256 devices in a mesh: ep: 64 (over z, y, core), tp: 4 (over x).
Axes of the slice: x: 4, y: 4, z: 8, core: 2. Of those that a mesh axis runs over, the one named last changes fastest.
Arguments:
- queries: bfloat16 [16384, 1024], P('ep', 'tp'), may hold values from -200 to 200
- keys: bfloat16 [16384, 512], P('ep', 'tp'), may hold values from -5 to 5
- values: bfloat16 [16384, 512], P('ep', 'tp'), may hold values from -6 to 6
- log_gates: float32 [16384, 16], P('ep', 'tp'), may hold values from -16384 to 0, as said below
- out_weight: bfloat16 [1024, 2048], P('tp'), may hold values from -0.1875 to 0.1875
- moe_rows: bfloat16 [16384, 2048], P('ep'), may hold values from -6 to 6
- norm_gain: float32 [2048], replicated, may hold values from 0.1 to 1.9
- experts: int32 [16384, 2], P('ep'), may hold values from 0 to 63, all different within a row; in each aligned block of 256 rows (0 to 255, 256 to 511, ...) at most 16 rows name the same one
- expert_weights: float32 [16384, 2], P('ep'), may hold values from 0.2 to 1
- w_gate: bfloat16 [64, 2048, 1024], P('ep', None, 'tp'), may hold values from -0.125 to 0.125
- w_up: bfloat16 [64, 2048, 1024], P('ep', None, 'tp'), may hold values from -0.125 to 0.125
- w_down: bfloat16 [64, 1024, 2048], P('ep', 'tp'), may hold values from -0.1875 to 0.1875
Outputs:
- mixed: bfloat16 [16384, 2048], P(('ep', 'tp'))
- moe_out: bfloat16 [16384, 2048], P('ep', 'tp')
The draws below stay inside these ranges and needn't reach their ends.
Inputs may be any that keep to these rules, and one draw needn't show every extreme that they name: Each token names 2 different experts; within the rows of one index of ep (aligned blocks of 256 rows) no expert is named more than 16 times, a bound that some block reaches. `log_gates`: Non-increasing along positions in every head.
All inputs are finite; a program needn't handle non-finite values.
Results may differ from the reference program's by a relative error of at most 0.01195.
Values may be sent and summed in bfloat16 or wider, within the bound.
No kernel may reach another device: no remote copies, remote signals or barrier semaphores. Data moves between devices by JAX's collectives and lax.ppermute only.
A program may use at most 128 MiB of HBM per device.

```python
import math
import jax
import jax.numpy as jnp
import numpy as np
from jax import lax

D = 2048
HD = 64
HEADS = 16
KV = 8
FF = 1024
TOPK = 2
TOK_DEV = 256
MOE_EP = 256
LEAD_SPAN_LENGTH = 16384
MTOK = 16384
EXPERTS = 64
CAP = 16
N_EP = 64
N_TP = 4


def attention_pair(key):
    reference_level = jax.random.fold_in(key, 11)
    query_key, key_key = jax.random.split(reference_level, 2)
    key_rows = jnp.clip(jax.random.normal(key_key, (LEAD_SPAN_LENGTH, KV * HD), jnp.float32), -5.0, 5.0)
    query_rows = jnp.clip(jax.random.normal(query_key, (LEAD_SPAN_LENGTH, HEADS * HD), jnp.float32), -5.0, 5.0)
    return (query_rows, key_rows)


def draw_queries(key, part):
    return attention_pair(key)[0].astype(jnp.bfloat16)


def draw_keys(key, part):
    return attention_pair(key)[1].astype(jnp.bfloat16)


def draw_log_gates(key, part):
    reference_level = jax.random.fold_in(key, 23)
    arrangement_prng_seed, iteration_prng_seed, tile_prng_seed, spike_prng_seed, objective_prng_seed = jax.random.split(reference_level, 5)
    head_rank = jax.random.permutation(arrangement_prng_seed, HEADS)
    delay_multiplier = head_rank < HEADS // 2
    per_step = jnp.exp(jax.random.uniform(iteration_prng_seed, (LEAD_SPAN_LENGTH, HEADS), jnp.float32, jnp.log(0.5), jnp.log(2.0)))
    block_factor = jnp.exp(jax.random.uniform(tile_prng_seed, (LEAD_SPAN_LENGTH // TOK_DEV, HEADS), jnp.float32, jnp.log(0.7), jnp.log(2.8)))
    block_factor = jnp.repeat(block_factor, TOK_DEV, axis=0)
    rate = jnp.where(delay_multiplier, 0.3 / LEAD_SPAN_LENGTH, 1.0 / 40.0)
    iteration_record = -rate[None, :] * per_step * block_factor
    spike_word_locations = jax.random.randint(spike_prng_seed, (3,), 0, LEAD_SPAN_LENGTH)
    objective_readings = jax.random.uniform(objective_prng_seed, (3, HEADS), jnp.float32, jnp.log(0.6), jnp.log(0.8))
    agreement_tally = (jnp.arange(LEAD_SPAN_LENGTH)[:, None] == spike_word_locations[None, :]).astype(jnp.float32)
    spike_addend = jnp.dot(agreement_tally, objective_readings)
    iteration_record = iteration_record + jnp.where(delay_multiplier[None, :], spike_addend, 0.0)
    return jnp.cumsum(iteration_record, axis=0)


def shard_levels(own_key, dims, shards, least, top_value):
    level = 1.0
    for dim, parts in shards:
        heights = jax.random.uniform(jax.random.fold_in(jax.random.fold_in(own_key, 6), dim), (parts,), jnp.float32, least / len(shards), top_value / len(shards))
        level = level * jnp.repeat(jnp.exp(heights), dims[dim] // parts).reshape((-1,) + (1,) * (len(dims) - 1 - dim))
    return level


def shared_out(stream_key, own, number, rows, number_of, top, most, slope):
    order = jax.random.permutation(stream_key, number_of)
    crowded, usual = load_shares(number_of, rows * top, most, slope, True), load_shares(number_of, rows * top, most, slope, False)
    places = jnp.arange(number_of)

    def named(sizes, offset_by):
        used = int((sizes > 0).sum())
        fixed = max(1, used // 4)
        moved = fixed + (places - fixed + offset_by * (used - fixed)) % max(1, number_of - fixed)
        return jnp.zeros((number_of,), jnp.int32).at[order[jnp.where(places < fixed, places, moved)]].set(jnp.asarray(sizes, jnp.int32))

    sizes = jnp.where(number % 4 == 0, named(crowded, number // 4), named(usual, number - number // 4 - 1))
    mixed = jax.random.permutation(jax.random.fold_in(own, 3), number_of)
    giver, taker = mixed[0:number_of // 2 * 2:2], mixed[1:number_of // 2 * 2:2]
    room = jnp.minimum(sizes[giver] - 1, most - sizes[taker]) // 2
    room = jnp.where((giver == order[0]) | (taker == order[0]) | (sizes[taker] == 0), 0, jnp.maximum(room, 0))
    moved = jax.random.randint(jax.random.fold_in(own, 4), (number_of // 2,), 0, 1 << 20) % (room + 1)
    sizes = sizes.at[giver].add(-moved).at[taker].add(moved)
    members = jnp.searchsorted(jnp.cumsum(sizes), jnp.arange(rows * top), side="right").astype(jnp.int32)
    grid = members.reshape(top, rows).T
    grid = grid[jax.random.permutation(jax.random.fold_in(own, 1), rows)]
    offset_by = jax.random.randint(jax.random.fold_in(own, 2), (rows, 1), 0, top)
    return jnp.take_along_axis(grid, (jnp.arange(top)[None, :] + offset_by) % top, axis=1)


def load_shares(amount, total, limit, slope, full):
    portions = [(1 << 20) // math.isqrt(grade ** slope) + 1 for grade in range(1, amount + 1)]
    largest = limit if full else min(limit, max(-(-total // amount), total * portions[0] // sum(portions)))
    least = 1 if total - largest >= amount - 1 else 0
    counts, spare = [largest] + [least] * (amount - 1), total - largest - least * (amount - 1)
    while spare > 0:
        candidates = [i for i in range(1, amount) if counts[i] < largest] or [i for i in range(1, amount) if counts[i] < limit]
        whole, remaining = sum([portions[i] for i in candidates]), spare
        for i in candidates:
            addition = min(limit - counts[i], max(1, remaining * portions[i] // whole), spare)
            counts[i] = counts[i] + addition
            spare = spare - addition
    return np.array(counts)


def centred(own_key, dims, scale, most, cuts=(), held_as=jnp.bfloat16):
    values = scale * jax.random.normal(own_key, dims, jnp.float32)
    if cuts:
        values = values * shard_levels(own_key, dims, cuts, -0.22, 0.18)
    return jnp.clip(values, -most, most).astype(held_as)


def setup_inputs(seed: int = 0) -> dict:
    seeds = jax.random.split(jax.random.key(seed), 13)
    queries = draw_queries(jax.random.fold_in(seeds[12], 71), 0)
    keys = draw_keys(jax.random.fold_in(seeds[12], 71), 0)
    values = centred(seeds[2], (LEAD_SPAN_LENGTH, KV * HD), 1.0, 6.0, ((0, 64), (1, 4)))
    log_gates = draw_log_gates(jax.random.fold_in(seeds[12], 71), 0)
    out_weight = centred(seeds[4], (HEADS * HD, D), (HEADS * HD) ** -0.5, 0.1875, ((0, 4),))
    moe_rows = centred(seeds[5], (MTOK, D), 1.0, 6.0, ((0, 64),))
    norm_gain = jnp.clip(1.0 + 0.18 * jax.random.normal(seeds[6], (D,), jnp.float32), 0.1, 1.9)
    experts_keys = jax.random.split(jax.random.fold_in(seeds[7], 1), MTOK // MOE_EP)
    experts_turns = jax.random.permutation(jax.random.fold_in(seeds[7], 3), MTOK // MOE_EP)
    experts = jax.vmap(lambda own, number: shared_out(jax.random.fold_in(seeds[7], 2), own, number, MOE_EP, EXPERTS, TOPK, CAP, 1))(experts_keys, experts_turns).reshape((MTOK, TOPK))
    expert_weights = jnp.clip(0.2 + 0.8 * jax.random.uniform(seeds[8], (MTOK, TOPK), jnp.float32) ** shard_levels(seeds[8], (MTOK, TOPK), ((0, 64),), -0.2, 0.2), 0.2, 1.0)
    w_gate = centred(seeds[9], (EXPERTS, D, FF), D ** -0.5, 0.125, ((0, 64), (2, 4)))
    w_up = centred(seeds[10], (EXPERTS, D, FF), D ** -0.5, 0.125, ((0, 64), (2, 4)))
    w_down = centred(seeds[11], (EXPERTS, FF, D), FF ** -0.5, 0.1875, ((0, 64), (1, 4)))
    return dict(queries=queries, keys=keys, values=values, log_gates=log_gates, out_weight=out_weight, moe_rows=moe_rows, norm_gain=norm_gain, experts=experts, expert_weights=expert_weights, w_gate=w_gate, w_up=w_up, w_down=w_down)


EPSILON = 1e-06

def split_sum(left, right, pieces):
    width = left.shape[1] // pieces
    total = jnp.zeros((left.shape[0], right.shape[1]), jnp.float32)
    for piece_index in range(pieces):
        partial_product = jnp.dot(left[:, piece_index * width:(piece_index + 1) * width], right[piece_index * width:(piece_index + 1) * width], preferred_element_type=jnp.float32)
        rounded = lax.optimization_barrier(partial_product.astype(jnp.bfloat16))
        total = total + rounded.astype(jnp.float32)
    return total.astype(jnp.bfloat16)

def reference(queries, keys, values, log_gates, out_weight, moe_rows, norm_gain, experts, expert_weights, w_gate, w_up, w_down):
    group = HEADS // KV
    query_heads = queries.reshape(LEAD_SPAN_LENGTH, KV, group, HD)
    key_heads = keys.reshape(LEAD_SPAN_LENGTH, KV, HD).astype(jnp.float32)
    value_heads = values.reshape(LEAD_SPAN_LENGTH, KV, HD).astype(jnp.float32)
    gate_lines = jnp.transpose(log_gates.reshape(LEAD_SPAN_LENGTH, KV, group), (1, 2, 0))
    query_span = math.gcd(LEAD_SPAN_LENGTH, 128)
    key_index = jnp.arange(LEAD_SPAN_LENGTH, dtype=jnp.int32)

    def attend(block_index):
        offset = block_index * query_span
        query_block = lax.dynamic_slice_in_dim(query_heads, offset, query_span, 0).astype(jnp.float32)
        query_gates = lax.dynamic_slice_in_dim(gate_lines, offset, query_span, 2)
        scores = jnp.einsum('qgrd,kgd->grqk', query_block, key_heads) * HD ** (-0.5)
        scores = scores + query_gates[..., None] - gate_lines[:, :, None, :]
        causal = key_index[None, :] <= (offset + jnp.arange(query_span, dtype=jnp.int32))[:, None]
        scores = jnp.where(causal, scores, -jnp.inf)
        highest = lax.optimization_barrier(jnp.max(scores, axis=-1, keepdims=True))
        weights = jnp.exp(scores - highest)
        totals = lax.optimization_barrier(jnp.sum(weights, axis=-1))
        rounded = lax.optimization_barrier(weights.astype(jnp.bfloat16)).astype(jnp.float32)
        heads_out = jnp.einsum('grqk,kgd->qgrd', rounded, value_heads)
        heads_out = heads_out / jnp.transpose(totals, (2, 0, 1))[..., None]
        return heads_out.reshape(query_span, HEADS * HD).astype(jnp.bfloat16)
    attended = lax.map(attend, jnp.arange(LEAD_SPAN_LENGTH // query_span, dtype=jnp.int32)).reshape(LEAD_SPAN_LENGTH, HEADS * HD)
    mixed = split_sum(attended, out_weight, N_TP)
    rows_float = moe_rows.astype(jnp.float32)
    normed = (rows_float * lax.rsqrt(lax.optimization_barrier(jnp.mean(rows_float * rows_float, axis=-1, keepdims=True)) + EPSILON) * norm_gain).astype(jnp.bfloat16)
    expert_ids = experts.reshape(N_EP, MOE_EP * TOPK)
    one_hot = (expert_ids[..., None] == jnp.arange(EXPERTS, dtype=jnp.int32)[None, None, :]).astype(jnp.int32)
    ranks = jnp.cumsum(one_hot, axis=1) - 1
    slot_index = lax.optimization_barrier(jnp.sum(one_hot * ranks, axis=-1)).astype(jnp.int32)
    source = jnp.arange(N_EP, dtype=jnp.int32)[:, None]
    destination = (expert_ids * (N_EP * CAP) + source * CAP + slot_index).reshape(-1).astype(jnp.int32)
    token_index = jnp.arange(MTOK * TOPK, dtype=jnp.int32) // TOPK
    buffer_rows = jnp.zeros((EXPERTS * N_EP * CAP, D), jnp.bfloat16).at[destination].set(normed[token_index])

    def run_expert(operands):
        rows, gate_weight, up_weight, down_weight = operands
        gate_part = jnp.dot(rows, gate_weight, preferred_element_type=jnp.float32)
        up_part = jnp.dot(rows, up_weight, preferred_element_type=jnp.float32)
        hidden = (jax.nn.silu(gate_part) * up_part).astype(jnp.bfloat16)
        return split_sum(hidden, down_weight, N_TP)
    results = lax.map(run_expert, (buffer_rows.reshape(EXPERTS, N_EP * CAP, D), w_gate, w_up, w_down))
    picked = results.reshape(EXPERTS * N_EP * CAP, D)[destination].reshape(MTOK, TOPK, D)
    moe_out = jnp.einsum('tk,tkd->td', expert_weights, picked.astype(jnp.float32)).astype(jnp.bfloat16)
    return (mixed, moe_out)
```

```python
import functools

import jax
import jax.numpy as jnp
from jax import lax
from jax.experimental import pallas as pl
from jax.experimental.pallas import tpu as pltpu
from jax.sharding import PartitionSpec as P

HD = 64
EPSILON = 1e-06
MASKED = -1e30
F32 = jnp.float32
BF16 = jnp.bfloat16
HEAD_ROWS = 80


def whole(shape):
    return pl.BlockSpec(shape, lambda *_: (0,) * len(shape))


def pack_body(keys_ref, values_ref, gates_ref, out_ref):
    rows = keys_ref.shape[0]
    half = rows // 2
    keys_t = keys_ref[...].astype(F32).T
    gates = gates_ref[...]
    high = gates.astype(BF16).astype(F32)
    rest = gates - high
    mid = rest.astype(BF16).astype(F32)
    low = rest - mid
    pad = jnp.zeros((10, rows), F32)
    for g in range(2):
        pieces = []
        for r in range(2):
            h = 2 * g + r
            pieces += [high[h : h + 1], mid[h : h + 1], low[h : h + 1]]
        block = jnp.concatenate([keys_t[g * HD : (g + 1) * HD]] + pieces + [pad], axis=0)
        out_ref[pl.ds(g * HEAD_ROWS, HEAD_ROWS), :] = block.astype(BF16)
    out_ref[pl.ds(2 * HEAD_ROWS, half), pl.ds(0, 128)] = values_ref[pl.ds(0, half), :]
    out_ref[pl.ds(2 * HEAD_ROWS, half), pl.ds(128, 128)] = values_ref[pl.ds(half, half), :]


def pack_keys(keys, values, gates_t):
    rows = keys.shape[0]
    height = 2 * HEAD_ROWS + rows // 2
    return pl.pallas_call(
        pack_body,
        out_shape=jax.ShapeDtypeStruct((height, rows), BF16),
        name="pack_keys",
    )(keys, values, gates_t)


def attention_body(index_ref, q_ref, kv_ref, w_ref, o_ref, qa_ref, acc_ref, max_ref, *, per_step):
    step = pl.program_id(0)
    own = index_ref[0]
    last = own // per_step
    rows = q_ref.shape[0]
    span = per_step * rows

    @pl.when(step == 0)
    def _():
        column = lax.broadcasted_iota(jnp.int32, (rows, 16), 1)
        for g in range(2):
            for r in range(2):
                h = 2 * g + r
                scaled = q_ref[:, h * HD : (h + 1) * HD].astype(F32) * HD ** (-0.5)
                picks = jnp.where((column >= 3 * r) & (column < 3 * r + 3), -1.0, 0.0)
                qa_ref[g, pl.ds(r * rows, rows), :] = jnp.concatenate(
                    [scaled, picks.astype(F32)], axis=1
                ).astype(BF16)
        acc_ref[...] = jnp.zeros_like(acc_ref)
        max_ref[...] = jnp.full_like(max_ref, MASKED)

    def run(masked):
        values = []
        for c in range(per_step):
            packed = kv_ref[c, pl.ds(2 * HEAD_ROWS, rows // 2), :]
            values += [packed[:, :128], packed[:, 128:]]
        values = jnp.concatenate(values, axis=0)
        values = jnp.concatenate([values, jnp.ones_like(values)], axis=1)
        for g in range(2):
            keys = jnp.concatenate(
                [kv_ref[c, pl.ds(g * HEAD_ROWS, HEAD_ROWS), :] for c in range(per_step)], axis=1
            )
            scores = jnp.dot(qa_ref[g], keys, preferred_element_type=F32)
            if masked:
                key_at = step * span + lax.broadcasted_iota(jnp.int32, scores.shape, 1)
                query_at = own * rows + lax.broadcasted_iota(jnp.int32, scores.shape, 0) % rows
                scores = jnp.where(key_at <= query_at, scores, MASKED)
            old = max_ref[g]
            new = jnp.maximum(old, jnp.max(scores, axis=1, keepdims=True))
            weights = jnp.exp(scores - new[:, :1]).astype(BF16)
            rescale = jnp.exp(old - new)
            max_ref[g] = new
            acc_ref[g] = acc_ref[g] * jnp.concatenate([rescale, rescale], axis=1) + jnp.dot(
                weights, values, preferred_element_type=F32
            )

    @pl.when(step < last)
    def _():
        run(False)

    @pl.when(step == last)
    def _():
        run(True)
        heads = []
        for g in range(2):
            done = acc_ref[g, :, :128] / acc_ref[g, :, 128:]
            for r in range(2):
                heads.append(done[r * rows : (r + 1) * rows, g * HD : (g + 1) * HD])
        attended = jnp.concatenate(heads, axis=1).astype(BF16)
        o_ref[...] = jnp.dot(attended, w_ref[...], preferred_element_type=F32).astype(BF16)


def attention(own_index, queries, packed, out_weight):
    parts, height, rows = packed.shape
    per_step = 4
    steps = parts // per_step
    wide = out_weight.shape[1]
    return pl.pallas_call(
        functools.partial(attention_body, per_step=per_step),
        grid_spec=pltpu.PrefetchScalarGridSpec(
            num_scalar_prefetch=1,
            grid=(steps,),
            in_specs=[
                whole(queries.shape),
                pl.BlockSpec(
                    (per_step, height, rows),
                    lambda s, own: (jnp.minimum(s, own[0] // per_step), 0, 0),
                ),
                whole(out_weight.shape),
            ],
            out_specs=whole((rows, wide)),
            scratch_shapes=[
                pltpu.VMEM((2, 2 * rows, HEAD_ROWS), BF16),
                pltpu.VMEM((2, 2 * rows, 256), F32),
                pltpu.VMEM((2, 2 * rows, 128), F32),
            ],
        ),
        out_shape=jax.ShapeDtypeStruct((rows, wide), BF16),
        compiler_params=pltpu.CompilerParams(dimension_semantics=("arbitrary",)),
        cost_estimate=pl.CostEstimate(
            flops=20_000_000_000, transcendentals=17_000_000, bytes_accessed=11_000_000
        ),
        name="attention",
    )(own_index, queries, packed, out_weight)


def mixer_half(queries, keys, values, log_gates, out_weight):
    packed = pack_keys(keys, values, log_gates.T)
    gathered = lax.all_gather(packed, "ep", axis=0, tiled=False)
    own_index = lax.axis_index("ep").astype(jnp.int32).reshape(1)
    partial = attention(own_index, queries, gathered, out_weight)
    return lax.psum_scatter(partial, "tp", scatter_dimension=0, tiled=True)


def dispatch_body(
    index_ref, rows_ref, part_ref, gain_ref, experts_t_ref, experts_ref, send_ref, slot_ref, *, cap
):
    tokens = rows_ref.shape[0]
    slots = send_ref.shape[0]
    count = slots // cap
    rows = rows_ref[...].astype(F32)
    scale = lax.rsqrt(jnp.mean(rows * rows, axis=1, keepdims=True) + EPSILON)
    normed = (part_ref[...].astype(F32) * scale * gain_ref[...]).astype(BF16)
    expert_at = lax.broadcasted_iota(jnp.int32, (count, tokens), 0)
    first = (expert_at == experts_t_ref[0:1, :]).astype(F32)
    second = (expert_at == experts_t_ref[1:2, :]).astype(F32)
    earlier = (
        lax.broadcasted_iota(jnp.int32, (tokens, tokens), 0)
        < lax.broadcasted_iota(jnp.int32, (tokens, tokens), 1)
    ).astype(BF16)
    base = (expert_at * cap).astype(F32)
    before_first = jnp.dot(first.astype(BF16), earlier, preferred_element_type=F32)
    before_second = jnp.dot(second.astype(BF16), earlier, preferred_element_type=F32) + jnp.sum(
        first, axis=1, keepdims=True
    )
    to_first = jnp.sum(first * (base + before_first), axis=0, keepdims=True).astype(jnp.int32)
    to_second = jnp.sum(second * (base + before_second), axis=0, keepdims=True).astype(jnp.int32)
    slot_at = lax.broadcasted_iota(jnp.int32, (slots, tokens), 0)
    chosen = ((slot_at == to_first) | (slot_at == to_second)).astype(F32).astype(BF16)
    send_ref[...] = jnp.dot(chosen, normed, preferred_element_type=F32).astype(BF16)
    expert_at = lax.broadcasted_iota(jnp.int32, (tokens, count), 1)
    first = (expert_at == experts_ref[:, 0:1]).astype(F32)
    second = (expert_at == experts_ref[:, 1:2]).astype(F32)
    earlier = (
        lax.broadcasted_iota(jnp.int32, (tokens, tokens), 1)
        < lax.broadcasted_iota(jnp.int32, (tokens, tokens), 0)
    ).astype(BF16)
    base = (expert_at * cap).astype(F32)
    before_first = jnp.dot(earlier, first.astype(BF16), preferred_element_type=F32)
    before_second = jnp.dot(earlier, second.astype(BF16), preferred_element_type=F32) + jnp.sum(
        first, axis=0, keepdims=True
    )
    to_first = jnp.sum(first * (base + before_first), axis=1, keepdims=True)
    to_second = jnp.sum(second * (base + before_second), axis=1, keepdims=True)
    slot_ref[:, 0:1] = to_first.astype(jnp.int32)
    slot_ref[:, 1:2] = to_second.astype(jnp.int32)


def dispatch(tp_index, moe_rows, norm_gain, experts, count, tp):
    tokens, width = moe_rows.shape
    cap = 4 * tokens // count
    part = width // tp
    return pl.pallas_call(
        functools.partial(dispatch_body, cap=cap),
        grid_spec=pltpu.PrefetchScalarGridSpec(
            num_scalar_prefetch=1,
            grid=(1,),
            in_specs=[
                whole(moe_rows.shape),
                pl.BlockSpec((tokens, part), lambda s, own: (0, own[0])),
                pl.BlockSpec((1, part), lambda s, own: (0, own[0])),
                whole((2, tokens)),
                whole((tokens, 2)),
            ],
            out_specs=[whole((count * cap, part)), whole((tokens, 2))],
        ),
        out_shape=[
            jax.ShapeDtypeStruct((count * cap, part), BF16),
            jax.ShapeDtypeStruct((tokens, 2), jnp.int32),
        ],
        name="dispatch",
    )(tp_index, moe_rows, moe_rows, norm_gain.reshape(1, -1), experts.T, experts)


def gather_over_tp(own):
    size = lax.axis_size("tp")
    up = [(n, (n + 1) % size) for n in range(size)]
    down = [(n, (n - 1) % size) for n in range(size)]
    half = own.shape[0] // 2
    previous = lax.ppermute(own, "tp", up)
    following = lax.ppermute(own, "tp", down)
    far_low = lax.ppermute(previous[:half], "tp", up)
    far_high = lax.ppermute(following[half:], "tp", down)
    return own, previous, following, far_low, far_high


def pick_parts(index_ref, refs, steps):
    own, previous, following, far_low, far_high = refs
    low = pl.program_id(0) < steps // 2
    tp = index_ref[0]
    return (
        (tp, own[...]),
        (lax.rem(tp + 3, 4), previous[...]),
        (lax.rem(tp + 1, 4), following[...]),
        (lax.rem(tp + 2, 4), jnp.where(low, far_low[...], far_high[...])),
    )


def part_specs(tall, wide, steps):
    block = tall // steps
    half = steps // 2
    straight = pl.BlockSpec((block, wide), lambda s, own: (s, 0))
    return [
        straight,
        straight,
        straight,
        pl.BlockSpec((block, wide), lambda s, own: (jnp.minimum(s, half - 1), 0)),
        pl.BlockSpec((block, wide), lambda s, own: (jnp.maximum(s - half, 0), 0)),
    ]


def up_body(index_ref, a, b, c, d, e, gate_ref, up_ref, out_ref, *, steps):
    gate = up = None
    for number, rows in pick_parts(index_ref, (a, b, c, d, e), steps):
        to_gate = jnp.dot(rows, gate_ref[number], preferred_element_type=F32)
        to_up = jnp.dot(rows, up_ref[number], preferred_element_type=F32)
        gate = to_gate if gate is None else gate + to_gate
        up = to_up if up is None else up + to_up
    out_ref[...] = (gate / (1.0 + jnp.exp(-gate)) * up).astype(BF16)


def up_projections(tp_index, parts, w_gate, w_up, tp):
    tall, wide = parts[0].shape
    steps = 4
    hidden = w_gate.shape[1]
    return pl.pallas_call(
        functools.partial(up_body, steps=steps),
        grid_spec=pltpu.PrefetchScalarGridSpec(
            num_scalar_prefetch=1,
            grid=(steps,),
            in_specs=part_specs(tall, wide, steps)
            + [whole((tp, wide, hidden)), whole((tp, wide, hidden))],
            out_specs=pl.BlockSpec((tall // steps, hidden), lambda s, own: (s, 0)),
        ),
        out_shape=jax.ShapeDtypeStruct((tall, hidden), BF16),
        cost_estimate=pl.CostEstimate(
            flops=2_200_000_000, transcendentals=262_144, bytes_accessed=6_800_000
        ),
        name="up_projections",
    )(tp_index, *parts, w_gate.reshape(tp, wide, hidden), w_up.reshape(tp, wide, hidden))


def down_body(index_ref, a, b, c, d, e, down_ref, out_ref, *, steps):
    total = None
    for number, rows in pick_parts(index_ref, (a, b, c, d, e), steps):
        term = jnp.dot(rows, down_ref[number], preferred_element_type=F32)
        total = term if total is None else total + term
    out_ref[...] = total.astype(BF16)


def down_projection(tp_index, parts, w_down, tp):
    tall, wide = parts[0].shape
    steps = 4
    columns = w_down.shape[1]
    return pl.pallas_call(
        functools.partial(down_body, steps=steps),
        grid_spec=pltpu.PrefetchScalarGridSpec(
            num_scalar_prefetch=1,
            grid=(steps,),
            in_specs=part_specs(tall, wide, steps) + [whole((tp, wide, columns))],
            out_specs=pl.BlockSpec((tall // steps, columns), lambda s, own: (s, 0)),
        ),
        out_shape=jax.ShapeDtypeStruct((tall, columns), BF16),
        cost_estimate=pl.CostEstimate(
            flops=1_100_000_000, transcendentals=0, bytes_accessed=4_200_000
        ),
        name="down_projection",
    )(tp_index, *parts, w_down.reshape(tp, wide, columns))


def combine_body(slot_ref, weight_ref, rows_ref, out_ref):
    slots = rows_ref.shape[0]
    tokens = slot_ref.shape[0]
    slot_at = lax.broadcasted_iota(jnp.int32, (tokens, slots), 1)
    total = None
    for k in range(2):
        chosen = (slot_at == slot_ref[:, k : k + 1]).astype(F32).astype(BF16)
        picked = jnp.dot(chosen, rows_ref[...], preferred_element_type=F32)
        term = picked * weight_ref[:, k : k + 1]
        total = term if total is None else total + term
    out_ref[...] = total.astype(BF16)


def combine(slots, expert_weights, rows):
    return pl.pallas_call(
        combine_body,
        out_shape=jax.ShapeDtypeStruct((slots.shape[0], rows.shape[1]), BF16),
        name="combine",
    )(slots, expert_weights, rows)


def experts_half(moe_rows, norm_gain, experts, expert_weights, w_gate, w_up, w_down):
    count = lax.axis_size("ep")
    tp = lax.axis_size("tp")
    tp_index = lax.axis_index("tp").astype(jnp.int32).reshape(1)
    down_columns = lax.all_to_all(w_down[0], "tp", split_axis=1, concat_axis=0, tiled=True)
    outgoing, slots = dispatch(tp_index, moe_rows, norm_gain, experts, count, tp)
    part = outgoing.shape[1]
    arrived = lax.all_to_all(
        outgoing.reshape(count, -1, part), "ep", split_axis=0, concat_axis=0, tiled=True
    ).reshape(-1, part)
    hidden = up_projections(tp_index, gather_over_tp(arrived), w_gate[0], w_up[0], tp)
    result = down_projection(tp_index, gather_over_tp(hidden), down_columns, tp)
    returned = lax.all_to_all(
        result.reshape(count, -1, part), "ep", split_axis=0, concat_axis=0, tiled=True
    ).reshape(-1, part)
    return combine(slots, expert_weights, returned)


def per_device(
    queries,
    keys,
    values,
    log_gates,
    out_weight,
    moe_rows,
    norm_gain,
    experts,
    expert_weights,
    w_gate,
    w_up,
    w_down,
):
    mixed = mixer_half(queries, keys, values, log_gates, out_weight)
    moe_out = experts_half(moe_rows, norm_gain, experts, expert_weights, w_gate, w_up, w_down)
    return (mixed, moe_out)


def solution(mesh):
    placed = (
        P("ep", "tp"),
        P("ep", "tp"),
        P("ep", "tp"),
        P("ep", "tp"),
        P("tp", None),
        P("ep", None),
        P(),
        P("ep", None),
        P("ep", None),
        P("ep", None, "tp"),
        P("ep", None, "tp"),
        P("ep", "tp", None),
    )
    return jax.shard_map(
        per_device,
        mesh=mesh,
        in_specs=placed,
        out_specs=(P(("ep", "tp"), None), P("ep", "tp")),
        check_vma=False,
    )
```

```python
import functools

import jax
import jax.numpy as jnp
from jax import lax
from jax.experimental import pallas as pl
from jax.experimental.pallas import tpu as pltpu
from jax.sharding import PartitionSpec as P


HD = 64
EPSILON = 1e-06
MASKED = -1e30
F32 = jnp.float32
BF16 = jnp.bfloat16
HEAD_ROWS = 80


def whole(shape):
    return pl.BlockSpec(shape, lambda *_: (0,) * len(shape))


def mirror_pairs(size):
    return [(n, size - 1 - n) for n in range(size)]


def along_z(shift, size):
    return [(n, (n + 8 * shift) % size) for n in range(size)]


def along_y(shift, size):
    return [(n, n // 8 * 8 + (n // 2 + shift) % 4 * 2 + n % 2) for n in range(size)]


Y_STEPS = (0, -1, 1, 2)
Z_STEPS = (0, -1, 1, -2, 2, -3, 3)
KV_ROWS = HEAD_ROWS + HD


def pieces_of(value):
    high = value.astype(BF16).astype(F32)
    rest = value - high
    mid = rest.astype(BF16).astype(F32)
    return high, mid, rest - mid


def pack_body(own_ref, queries_ref, keys_ref, values_ref, gates_ref, keep_ref, send_ref):
    rows = keys_ref.shape[0]
    keys_t = keys_ref[...].astype(F32).T
    values_t = values_ref[...].astype(F32).T
    queries_t = (queries_ref[...].astype(F32) * HD ** (-0.5)).T
    split = pieces_of(gates_ref[...])
    pad = jnp.zeros((HEAD_ROWS - HD - 6, rows), F32)
    blocks = []
    for g in range(2):
        gates = [piece[2 * g + r : 2 * g + r + 1] for r in range(2) for piece in split]
        heads = slice(g * HD, (g + 1) * HD)
        parts = [keys_t[heads]] + gates + [pad, values_t[heads]]
        parts.append(queries_t[2 * g * HD : 2 * (g + 1) * HD])
        blocks.append(jnp.concatenate(parts, axis=0).astype(BF16))
    even = lax.rem(own_ref[0], 2) == 0

    @pl.when(even)
    def _():
        keep_ref[...] = blocks[0]
        send_ref[...] = blocks[1]

    @pl.when(jnp.logical_not(even))
    def _():
        keep_ref[...] = blocks[1]
        send_ref[...] = blocks[0]


def pack(own, queries, keys, values, gates_t):
    rows = keys.shape[0]
    shape = (KV_ROWS + 2 * HD, rows)
    return pl.pallas_call(
        pack_body,
        grid_spec=pltpu.PrefetchScalarGridSpec(
            num_scalar_prefetch=1,
            grid=(1,),
            in_specs=[whole(x.shape) for x in (queries, keys, values, gates_t)],
            out_specs=[whole(shape), whole(shape)],
        ),
        out_shape=[jax.ShapeDtypeStruct(shape, BF16)] * 2,
        name="pack",
    )(own, queries, keys, values, gates_t)


def assemble_body(own_ref, *refs):
    kv_refs, key_ref, value_ref = refs[:9], refs[9], refs[10]
    z = own_ref[0] // 8
    rows = kv_refs[0].shape[2]
    value_ref[:, pl.ds(HD, HEAD_ROWS - HD), :] = jnp.ones(
        (value_ref.shape[0], HEAD_ROWS - HD, 2 * rows), BF16
    )

    def place_keys(slab, at, block):
        turned = block[:HEAD_ROWS].astype(F32).T
        key_ref[slab, pl.ds(at * rows, rows), :] = turned.astype(BF16)
        value_ref[slab, pl.ds(0, HD), pl.ds(at * rows, rows)] = block[HEAD_ROWS:]

    for number, shift in enumerate(Z_STEPS):
        source = lax.rem(z + shift + 8, 8)
        place_keys(source, 0, kv_refs[number][0])
        place_keys(7 - source, 1, kv_refs[number][1])
    source = lax.rem(z + 4, 8)
    place_keys(source, 0, kv_refs[7][0])
    place_keys(7 - source, 1, kv_refs[8][0])


def assemble(own, kv_parts):
    rows = kv_parts[0].shape[2]
    shapes = [(8, 2 * rows, HEAD_ROWS), (8, HEAD_ROWS, 2 * rows)]
    return pl.pallas_call(
        assemble_body,
        grid_spec=pltpu.PrefetchScalarGridSpec(
            num_scalar_prefetch=1,
            grid=(1,),
            in_specs=[whole(x.shape) for x in kv_parts],
            out_specs=[whole(shape) for shape in shapes],
        ),
        out_shape=[jax.ShapeDtypeStruct(shape, BF16) for shape in shapes],
        name="assemble",
    )(own, *kv_parts)


def attention_body(own_ref, *refs, steps):
    count_y = len(steps)
    q_refs, (key_ref, value_ref) = refs[:count_y], refs[count_y : count_y + 2]
    o_refs = refs[count_y + 2 : 2 * count_y + 2]
    query_ref, acc_ref, max_ref = refs[2 * count_y + 2 :]
    z, y, core = own_ref[0] // 8, own_ref[0] // 2 % 4, own_ref[0] % 2
    rows = q_refs[0].shape[2]
    line = lax.broadcasted_iota(jnp.int32, (HEAD_ROWS - HD, rows), 0)
    for number, ref in enumerate(q_refs):
        for slot in range(2):
            for r in range(2):
                picks = jnp.where((line >= 3 * r) & (line < 3 * r + 3), -1.0, 0.0).astype(F32)
                heads = ref[slot, r * HD : (r + 1) * HD, :].astype(F32)
                query_ref[2 * number + slot, r] = jnp.concatenate([heads, picks], axis=0).astype(
                    BF16
                )
    low = jnp.minimum(z, 7 - z)
    offset = 2 * y + core

    def run_half(high, carry):
        count = jnp.where(high == 1, 7 - low, low)
        slot = jnp.where(count == z, 0, 1)
        acc_ref[...] = jnp.zeros_like(acc_ref)
        max_ref[...] = jnp.full_like(max_ref, MASKED)

        def one_slab(slab, masked):
            keys = key_ref[slab]
            values = value_ref[slab]
            for number, shift in enumerate(steps):
                for r in range(2):
                    scores = jnp.dot(
                        keys, query_ref[2 * number + slot, r], preferred_element_type=F32
                    )
                    if masked:
                        line = lax.broadcasted_iota(jnp.int32, scores.shape, 0)
                        key_at = line + jnp.where(
                            line < rows, offset * rows, (7 - offset) * rows - rows
                        )
                        own = 2 * lax.rem(y + shift + 4, 4) + core
                        own = jnp.where(slot == 0, own, 7 - own)
                        query_at = own * rows + lax.broadcasted_iota(jnp.int32, scores.shape, 1)
                        scores = jnp.where(key_at <= query_at, scores, MASKED)
                    old = max_ref[number, r]
                    new = jnp.maximum(old, jnp.max(scores, axis=0, keepdims=True))
                    weights = jnp.exp(scores - new[0:1]).astype(BF16)
                    max_ref[number, r] = new
                    acc_ref[number, r] = acc_ref[number, r] * jnp.exp(old - new)[0:1] + jnp.dot(
                        values, weights, preferred_element_type=F32
                    )

        def open_slab(slab, carry):
            one_slab(slab, False)
            return carry

        lax.fori_loop(0, count, open_slab, 0)
        one_slab(count, True)
        blank = jnp.zeros((HEAD_ROWS - HD - 3, rows), F32)
        for number in range(count_y):
            for r in range(2):
                total = acc_ref[number, r]
                weight = total[HD : HD + 1]
                stats = pieces_of(max_ref[number, r][0:1] + jnp.log(weight))
                o_refs[number][slot, pl.ds(r * HEAD_ROWS, HEAD_ROWS), :] = jnp.concatenate(
                    [total[:HD] / weight, *stats, blank], axis=0
                ).astype(BF16)
        return carry

    lax.fori_loop(0, 2, run_half, 0)


def attention(own, steps, query_parts, keys, values):
    rows = query_parts[0].shape[2]
    count_y = len(steps)
    shape = (2, 2 * HEAD_ROWS, rows)
    operands = (*query_parts, keys, values)
    return pl.pallas_call(
        functools.partial(attention_body, steps=steps),
        grid_spec=pltpu.PrefetchScalarGridSpec(
            num_scalar_prefetch=1,
            grid=(1,),
            in_specs=[whole(x.shape) for x in operands],
            out_specs=[whole(shape)] * count_y,
            scratch_shapes=[
                pltpu.VMEM((2 * count_y, 2, HEAD_ROWS, rows), BF16),
                pltpu.VMEM((count_y, 2, HEAD_ROWS, rows), F32),
                pltpu.VMEM((count_y, 2, 8, rows), F32),
            ],
        ),
        out_shape=[jax.ShapeDtypeStruct(shape, BF16)] * count_y,
        cost_estimate=pl.CostEstimate(
            flops=10_000_000_000, transcendentals=5_000_000, bytes_accessed=2_000_000
        ),
        name="attention",
    )(own, *operands)


def merge_body(a, b, c, d, keep_ref, send_ref):
    for slot, target in enumerate((keep_ref, send_ref)):
        heads = []
        for r in range(2):
            block = pl.ds(r * HEAD_ROWS, HEAD_ROWS)
            parts = [ref[slot, block, :].astype(F32) for ref in (a, b, c, d)]
            logs = [x[HD : HD + 1] + x[HD + 1 : HD + 2] + x[HD + 2 : HD + 3] for x in parts]
            highest = functools.reduce(jnp.maximum, logs)
            shares = [jnp.exp(x - highest) for x in logs]
            total = functools.reduce(jnp.add, shares)
            mixed = functools.reduce(
                jnp.add, [x[:HD] * share for x, share in zip(parts, shares)]
            )
            heads.append(mixed / total)
        target[...] = jnp.concatenate(heads, axis=0).T.astype(BF16)


def merge(parts):
    rows = parts[0].shape[2]
    return pl.pallas_call(
        merge_body,
        out_shape=[jax.ShapeDtypeStruct((rows, 2 * HD), BF16)] * 2,
        name="merge",
    )(*parts)


def project_body(own_ref, tp_ref, keep_ref, back_ref, w_ref, *out_refs):
    tp = len(out_refs)
    even = lax.rem(own_ref[0], 2) == 0
    rows = out_refs[0].shape[0]
    for shift, ref in enumerate(out_refs):
        at = pl.multiple_of(lax.rem(tp_ref[0] + shift, tp) * rows, rows)
        kept, back = keep_ref[pl.ds(at, rows), :], back_ref[pl.ds(at, rows), :]
        attended = jnp.concatenate(
            [jnp.where(even, kept, back), jnp.where(even, back, kept)], axis=1
        )
        ref[...] = jnp.dot(attended, w_ref[...], preferred_element_type=F32).astype(BF16)


def project(own, tp_index, keep, back, out_weight, tp):
    shape = (keep.shape[0] // tp, out_weight.shape[1])
    return pl.pallas_call(
        project_body,
        grid_spec=pltpu.PrefetchScalarGridSpec(
            num_scalar_prefetch=2,
            grid=(1,),
            in_specs=[whole(x.shape) for x in (keep, back, out_weight)],
            out_specs=[whole(shape)] * tp,
        ),
        out_shape=[jax.ShapeDtypeStruct(shape, BF16)] * tp,
        name="project",
    )(own, tp_index, keep, back, out_weight)


CHUNKS = 1


def slot_number(named, rank, expert_at, cap, chunk, axis):
    part = cap // CHUNKS
    base = (expert_at * part).astype(F32)
    number = base + rank
    for cut in range(1, CHUNKS):
        number = number + jnp.where(rank >= cut * part, float(chunk - part), 0.0)
    return jnp.sum(named * number, axis=axis, keepdims=True).astype(jnp.int32)


def dispatch_body(
    index_ref, rows_ref, part_ref, gain_ref, experts_t_ref, *send_refs, cap
):
    tokens = rows_ref.shape[0]
    chunk = send_refs[0].shape[0]
    slots = chunk * len(send_refs)
    count = slots // cap
    rows = rows_ref[...].astype(F32)
    scale = lax.rsqrt(jnp.mean(rows * rows, axis=1, keepdims=True) + EPSILON)
    normed = (part_ref[...].astype(F32) * scale * gain_ref[...]).astype(BF16)
    expert_at = lax.broadcasted_iota(jnp.int32, (count, tokens), 0)
    first = (expert_at == experts_t_ref[0:1, :]).astype(F32)
    second = (expert_at == experts_t_ref[1:2, :]).astype(F32)
    earlier = (
        lax.broadcasted_iota(jnp.int32, (tokens, tokens), 0)
        < lax.broadcasted_iota(jnp.int32, (tokens, tokens), 1)
    ).astype(BF16)
    before_first = jnp.dot(first.astype(BF16), earlier, preferred_element_type=F32)
    before_second = jnp.dot(second.astype(BF16), earlier, preferred_element_type=F32) + jnp.sum(
        first, axis=1, keepdims=True
    )
    to_first = slot_number(first, before_first, expert_at, cap, chunk, 0)
    to_second = slot_number(second, before_second, expert_at, cap, chunk, 0)
    slot_at = lax.broadcasted_iota(jnp.int32, (slots, tokens), 0)
    chosen = ((slot_at == to_first) | (slot_at == to_second)).astype(F32).astype(BF16)
    for number, ref in enumerate(send_refs):
        picks = chosen[number * chunk : (number + 1) * chunk]
        ref[...] = jnp.dot(picks, normed, preferred_element_type=F32).astype(BF16)


def dispatch(tp_index, moe_rows, norm_gain, experts, count, tp):
    tokens, width = moe_rows.shape
    cap = 4 * tokens // count
    part = width // tp
    return pl.pallas_call(
        functools.partial(dispatch_body, cap=cap),
        grid_spec=pltpu.PrefetchScalarGridSpec(
            num_scalar_prefetch=1,
            grid=(1,),
            in_specs=[
                whole(moe_rows.shape),
                pl.BlockSpec((tokens, part), lambda s, own: (0, own[0])),
                pl.BlockSpec((1, part), lambda s, own: (0, own[0])),
                whole((2, tokens)),
            ],
            out_specs=[whole((count * cap // CHUNKS, part))] * CHUNKS,
        ),
        out_shape=[jax.ShapeDtypeStruct((count * cap // CHUNKS, part), BF16)] * CHUNKS,
        name="dispatch",
    )(tp_index, moe_rows, moe_rows, norm_gain.reshape(1, -1), experts.T)


def way_back_body(experts_ref, slot_ref, *, count, cap):
    tokens = experts_ref.shape[0]
    expert_at = lax.broadcasted_iota(jnp.int32, (tokens, count), 1)
    first = (expert_at == experts_ref[:, 0:1]).astype(F32)
    second = (expert_at == experts_ref[:, 1:2]).astype(F32)
    earlier = (
        lax.broadcasted_iota(jnp.int32, (tokens, tokens), 1)
        < lax.broadcasted_iota(jnp.int32, (tokens, tokens), 0)
    ).astype(BF16)
    before_first = jnp.dot(earlier, first.astype(BF16), preferred_element_type=F32)
    before_second = jnp.dot(earlier, second.astype(BF16), preferred_element_type=F32) + jnp.sum(
        first, axis=0, keepdims=True
    )
    chunk = count * cap // CHUNKS
    slot_ref[:, 0:1] = slot_number(first, before_first, expert_at, cap, chunk, 1)
    slot_ref[:, 1:2] = slot_number(second, before_second, expert_at, cap, chunk, 1)


def way_back(experts, count):
    cap = 4 * experts.shape[0] // count
    return pl.pallas_call(
        functools.partial(way_back_body, count=count, cap=cap),
        out_shape=jax.ShapeDtypeStruct(experts.shape, jnp.int32),
        name="way_back",
    )(experts)


def pick_parts(index_ref, refs, steps):
    own, previous, following, far_low, far_high = refs
    low = pl.program_id(0) < steps // 2
    tp = index_ref[0]
    return (
        (tp, own[...]),
        (lax.rem(tp + 3, 4), previous[...]),
        (lax.rem(tp + 1, 4), following[...]),
        (lax.rem(tp + 2, 4), jnp.where(low, far_low[...], far_high[...])),
    )


def part_specs(tall, wide, steps):
    block = tall // steps
    half = steps // 2
    straight = pl.BlockSpec((block, wide), lambda s, own: (s, 0))
    return [
        straight,
        straight,
        straight,
        pl.BlockSpec((block, wide), lambda s, own: (jnp.minimum(s, half - 1), 0)),
        pl.BlockSpec((block, wide), lambda s, own: (jnp.maximum(s - half, 0), 0)),
    ]


def up_body(index_ref, a, b, c, d, e, gate_ref, up_ref, out_ref, *, steps):
    gate = up = None
    for number, rows in pick_parts(index_ref, (a, b, c, d, e), steps):
        to_gate = jnp.dot(rows, gate_ref[number], preferred_element_type=F32)
        to_up = jnp.dot(rows, up_ref[number], preferred_element_type=F32)
        gate = to_gate if gate is None else gate + to_gate
        up = to_up if up is None else up + to_up
    out_ref[...] = (gate / (1.0 + jnp.exp(-gate)) * up).astype(BF16)


def up_projections(tp_index, parts, w_gate, w_up, tp):
    tall, wide = parts[0].shape
    steps = 4
    hidden = w_gate.shape[1]
    return pl.pallas_call(
        functools.partial(up_body, steps=steps),
        grid_spec=pltpu.PrefetchScalarGridSpec(
            num_scalar_prefetch=1,
            grid=(steps,),
            in_specs=part_specs(tall, wide, steps)
            + [whole((tp, wide, hidden)), whole((tp, wide, hidden))],
            out_specs=pl.BlockSpec((tall // steps, hidden), lambda s, own: (s, 0)),
        ),
        out_shape=jax.ShapeDtypeStruct((tall, hidden), BF16),
        cost_estimate=pl.CostEstimate(
            flops=2_200_000_000, transcendentals=262_144, bytes_accessed=6_800_000
        ),
        name="up_projections",
    )(tp_index, *parts, w_gate.reshape(tp, wide, hidden), w_up.reshape(tp, wide, hidden))


def down_body(index_ref, a, b, c, d, e, own_w, previous_w, following_w, far_w, out_ref, *, steps):
    low = pl.program_id(0) < steps // 2
    far_rows = jnp.where(low, d[...], e[...])
    total = jnp.dot(a[...], own_w[...], preferred_element_type=F32)
    total = total + jnp.dot(b[...], previous_w[...], preferred_element_type=F32)
    total = total + jnp.dot(c[...], following_w[...], preferred_element_type=F32)
    total = total + jnp.dot(far_rows, far_w[...], preferred_element_type=F32)
    out_ref[...] = total.astype(BF16)


def down_projection(tp_index, parts, w_down, moved):
    tall, wide = parts[0].shape
    steps = 4
    columns = moved[0].shape[1]
    return pl.pallas_call(
        functools.partial(down_body, steps=steps),
        grid_spec=pltpu.PrefetchScalarGridSpec(
            num_scalar_prefetch=1,
            grid=(steps,),
            in_specs=part_specs(tall, wide, steps)
            + [pl.BlockSpec((wide, columns), lambda s, own: (0, own[0]))]
            + [whole((wide, columns))] * 3,
            out_specs=pl.BlockSpec((tall // steps, columns), lambda s, own: (s, 0)),
        ),
        out_shape=jax.ShapeDtypeStruct((tall, columns), BF16),
        cost_estimate=pl.CostEstimate(
            flops=1_100_000_000, transcendentals=0, bytes_accessed=4_200_000
        ),
        name="down_projection",
    )(tp_index, *parts, w_down, *moved)


def cut_body(index_ref, a, b, c, to_a, to_b, to_c):
    to_a[...] = a[...]
    to_b[...] = b[...]
    to_c[...] = c[...]


def cut_columns(tp_index, w_down, tp):
    wide, columns = w_down.shape[0], w_down.shape[1] // tp

    def block(shift):
        return pl.BlockSpec((wide, columns), lambda s, own: (0, lax.rem(own[0] + shift, tp)))

    return pl.pallas_call(
        cut_body,
        grid_spec=pltpu.PrefetchScalarGridSpec(
            num_scalar_prefetch=1,
            grid=(1,),
            in_specs=[block(1), block(tp - 1), block(2)],
            out_specs=[whole((wide, columns))] * 3,
        ),
        out_shape=[jax.ShapeDtypeStruct((wide, columns), BF16)] * 3,
        name="cut_columns",
    )(tp_index, w_down, w_down, w_down)


def combine_body(slot_ref, weight_ref, *refs):
    row_refs, out_ref = refs[:-1], refs[-1]
    chunk = row_refs[0].shape[0]
    tokens = slot_ref.shape[0]
    total = None
    for k in range(2):
        picked = None
        for number, ref in enumerate(row_refs):
            slot_at = number * chunk + lax.broadcasted_iota(jnp.int32, (tokens, chunk), 1)
            chosen = (slot_at == slot_ref[:, k : k + 1]).astype(F32).astype(BF16)
            found = jnp.dot(chosen, ref[...], preferred_element_type=F32)
            picked = found if picked is None else picked + found
        term = picked * weight_ref[:, k : k + 1]
        total = term if total is None else total + term
    out_ref[...] = total.astype(BF16)


def combine(slots, expert_weights, rows):
    return pl.pallas_call(
        combine_body,
        out_shape=jax.ShapeDtypeStruct((slots.shape[0], rows[0].shape[1]), BF16),
        name="combine",
    )(slots, expert_weights, *rows)


def per_device(
    queries,
    keys,
    values,
    log_gates,
    out_weight,
    moe_rows,
    norm_gain,
    experts,
    expert_weights,
    w_gate,
    w_up,
    w_down,
):
    size = lax.axis_size("ep")
    tp = lax.axis_size("tp")
    own = lax.axis_index("ep").astype(jnp.int32).reshape(1)
    tp_index = lax.axis_index("tp").astype(jnp.int32).reshape(1)
    up_ring = [(n, (n + 1) % tp) for n in range(tp)]
    down_ring = [(n, (n - 1) % tp) for n in range(tp)]

    def over_ep(x):
        wide = x.shape[1]
        moved = lax.all_to_all(
            x.reshape(size, -1, wide), "ep", split_axis=0, concat_axis=0, tiled=True
        )
        return moved.reshape(-1, wide)

    def near(x):
        return lax.ppermute(x, "tp", up_ring), lax.ppermute(x, "tp", down_ring)

    def far(pair):
        half = pair[0].shape[0] // 2
        low, high = pair[0][:half], pair[1][half:]
        return lax.ppermute(low, "tp", up_ring), lax.ppermute(high, "tp", down_ring)

    keep, send = pack(own, queries, keys, values, log_gates.T)
    mirrored = lax.ppermute(send, "ep", mirror_pairs(size))
    outgoing = dispatch(tp_index, moe_rows, norm_gain, experts, size, tp)
    arrived = []
    for rows in outgoing:
        arrived.append(over_ep(rows))
    both = jnp.stack([keep, mirrored])
    own_keys, own_queries = both[:, :KV_ROWS], both[:, KV_ROWS:]
    query_parts = [own_queries] + [
        lax.ppermute(own_queries, "ep", along_y(-step, size)) for step in Y_STEPS[1:]
    ]
    below2, above2, below, above = [
        lax.ppermute(own_keys, "ep", along_z(shift, size)) for shift in (2, -2, 1, -1)
    ]
    below3 = lax.ppermute(below2, "ep", along_z(1, size))
    above3 = lax.ppermute(above2, "ep", along_z(-1, size))
    far_low = lax.ppermute(below2[:1], "ep", along_z(2, size))
    far_high = lax.ppermute(above2[1:], "ep", along_z(-2, size))
    kv_parts = [own_keys, below, above, below2, above2, below3, above3, far_low, far_high]
    slab_keys, slab_values = assemble(own, kv_parts)
    far_ring = [(n, (n + 2) % tp) for n in range(tp)]
    cuts = cut_columns(tp_index, w_down[0], tp)
    moved = [
        lax.ppermute(cut, "tp", ring) for cut, ring in zip(cuts, (up_ring, down_ring, far_ring))
    ]
    slots = way_back(experts, size)
    x_near = [near(rows) for rows in arrived]
    x_far = [far(pair) for pair in x_near]
    partial = {}
    for picks in ((3, 1), (2, 0)):
        done = attention(
            own,
            tuple(Y_STEPS[n] for n in picks),
            [query_parts[n] for n in picks],
            slab_keys,
            slab_values,
        )
        for n, part in zip(picks, done):
            if n:
                part = lax.ppermute(part, "ep", along_y(Y_STEPS[n], size))
            partial[n] = part
    h_near, h_far, hidden = [], [], []
    for number in range(CHUNKS):
        hidden.append(
            up_projections(
                tp_index,
                (arrived[number],) + x_near[number] + x_far[number],
                w_gate[0],
                w_up[0],
                tp,
            )
        )
        h_near.append(near(hidden[number]))
        h_far.append(far(h_near[number]))
    kept, sent = merge([partial[n] for n in range(4)])
    back = lax.ppermute(sent, "ep", mirror_pairs(size))
    products = project(own, tp_index, kept, back, out_weight, tp)
    others = [
        lax.ppermute(product, "tp", ring)
        for product, ring in zip(products[1:], (up_ring, far_ring, down_ring))
    ]
    mixed = sum(part.astype(F32) for part in [products[0]] + others).astype(BF16)
    returned = []
    for number in range(CHUNKS):
        result = down_projection(
            tp_index, (hidden[number],) + h_near[number] + h_far[number], w_down[0], moved
        )
        returned.append(over_ep(result))
    moe_out = combine(slots, expert_weights, returned)
    return (mixed, moe_out)


def solution(mesh):
    placed = (
        P("ep", "tp"),
        P("ep", "tp"),
        P("ep", "tp"),
        P("ep", "tp"),
        P("tp", None),
        P("ep", None),
        P(),
        P("ep", None),
        P("ep", None),
        P("ep", None, "tp"),
        P("ep", None, "tp"),
        P("ep", "tp", None),
    )
    return jax.shard_map(
        per_device,
        mesh=mesh,
        in_specs=placed,
        out_specs=(P(("ep", "tp"), None), P("ep", "tp")),
        check_vma=False,
    )
```

```python
import functools

import jax
import jax.numpy as jnp
from jax import lax
from jax.experimental import pallas as pl
from jax.experimental.pallas import tpu as pltpu
from jax.sharding import PartitionSpec as P


HD = 64
EPSILON = 1e-06
MASKED = -1e30
F32 = jnp.float32
BF16 = jnp.bfloat16
HEAD_ROWS = 80


def whole(shape):
    return pl.BlockSpec(shape, lambda *_: (0,) * len(shape))


def mirror_pairs(size):
    return [(n, size - 1 - n) for n in range(size)]


def along_z(shift, size):
    return [(n, (n + 8 * shift) % size) for n in range(size)]


def along_y(shift, size):
    return [(n, n // 8 * 8 + (n // 2 + shift) % 4 * 2 + n % 2) for n in range(size)]


Y_STEPS = (0, -1, 1, 2)
Z_STEPS = (0, -1, 1, -2, 2, -3, 3)
KV_ROWS = HEAD_ROWS + HD


def pieces_of(value):
    high = value.astype(BF16).astype(F32)
    rest = value - high
    mid = rest.astype(BF16).astype(F32)
    return high, mid, rest - mid


def pack_body(own_ref, queries_ref, keys_ref, values_ref, gates_ref, keep_ref, send_ref):
    rows = keys_ref.shape[0]
    half = rows // 2
    keys_t = keys_ref[...].astype(F32).T
    values_t = values_ref[...].astype(F32).T
    split = pieces_of(gates_ref[...])
    pad = jnp.zeros((HEAD_ROWS - HD - 6, rows), F32)
    blocks = []
    for g in range(2):
        gates = [piece[2 * g + r : 2 * g + r + 1] for r in range(2) for piece in split]
        heads = slice(g * HD, (g + 1) * HD)
        upper = jnp.concatenate([keys_t[heads]] + gates + [pad, values_t[heads]], axis=0)
        wide = queries_ref[:, g * 128 : (g + 1) * 128].astype(F32)
        lower = jnp.concatenate([wide[:half], wide[half:]], axis=1)
        blocks.append(jnp.concatenate([upper, lower], axis=0).astype(BF16))
    even = lax.rem(own_ref[0], 2) == 0

    @pl.when(even)
    def _():
        keep_ref[...] = blocks[0]
        send_ref[...] = blocks[1]

    @pl.when(jnp.logical_not(even))
    def _():
        keep_ref[...] = blocks[1]
        send_ref[...] = blocks[0]


def pack(own, queries, keys, values, gates_t):
    rows = keys.shape[0]
    shape = (KV_ROWS + rows // 2, rows)
    return pl.pallas_call(
        pack_body,
        grid_spec=pltpu.PrefetchScalarGridSpec(
            num_scalar_prefetch=1,
            grid=(1,),
            in_specs=[whole(x.shape) for x in (queries, keys, values, gates_t)],
            out_specs=[whole(shape), whole(shape)],
        ),
        out_shape=[jax.ShapeDtypeStruct(shape, BF16)] * 2,
        name="pack",
    )(own, queries, keys, values, gates_t)


def assemble_body(own_ref, *refs):
    kv_refs, key_ref, value_ref = refs[:9], refs[9], refs[10]
    z = own_ref[0] // 8
    rows = kv_refs[0].shape[2]
    ones = jnp.ones((rows, HD), F32)

    def place_keys(slab, at, block):
        key_ref[slab, :, pl.ds(at * rows, rows)] = block[:HEAD_ROWS]
        turned = block[HEAD_ROWS:].astype(F32).T
        value_ref[slab, pl.ds(at * rows, rows), :] = jnp.concatenate(
            [turned, ones], axis=1
        ).astype(BF16)

    for number, shift in enumerate(Z_STEPS):
        source = lax.rem(z + shift + 8, 8)
        place_keys(source, 0, kv_refs[number][0])
        place_keys(7 - source, 1, kv_refs[number][1])
    source = lax.rem(z + 4, 8)
    place_keys(source, 0, kv_refs[7][0])
    place_keys(7 - source, 1, kv_refs[8][0])


def assemble(own, kv_parts):
    rows = kv_parts[0].shape[2]
    shapes = [(8, HEAD_ROWS, 2 * rows), (8, 2 * rows, 128)]
    return pl.pallas_call(
        assemble_body,
        grid_spec=pltpu.PrefetchScalarGridSpec(
            num_scalar_prefetch=1,
            grid=(1,),
            in_specs=[whole(x.shape) for x in kv_parts],
            out_specs=[whole(shape) for shape in shapes],
        ),
        out_shape=[jax.ShapeDtypeStruct(shape, BF16) for shape in shapes],
        name="assemble",
    )(own, *kv_parts)


def attention_body(own_ref, *refs, steps):
    count_y = len(steps)
    q_refs, (key_ref, value_ref) = refs[:count_y], refs[count_y : count_y + 2]
    o_refs = refs[count_y + 2 : 2 * count_y + 2]
    query_ref, acc_ref, max_ref, score_ref = refs[2 * count_y + 2 :]
    z, y, core = own_ref[0] // 8, own_ref[0] // 2 % 4, own_ref[0] % 2
    rows = q_refs[0].shape[2]
    column = lax.broadcasted_iota(jnp.int32, (rows, HEAD_ROWS - HD), 1)
    for number, ref in enumerate(q_refs):
        for slot in range(2):
            packed = ref[slot].astype(F32) * HD ** (-0.5)
            both = jnp.concatenate([packed[:, :128], packed[:, 128:]], axis=0)
            for r in range(2):
                picks = jnp.where((column >= 3 * r) & (column < 3 * r + 3), -1.0, 0.0)
                query_ref[slot, pl.ds((2 * number + r) * rows, rows), :] = jnp.concatenate(
                    [both[:, r * HD : (r + 1) * HD], picks.astype(F32)], axis=1
                ).astype(BF16)
    low = jnp.minimum(z, 7 - z)
    offset = 2 * y + core

    blocks = range(0, 2 * count_y * rows, TALL)

    def run_half(high, carry):
        count = jnp.where(high == 1, 7 - low, low)
        slot = jnp.where(count == z, 0, 1)
        for block in blocks:
            at = pl.ds(block, TALL)
            scores = jnp.dot(query_ref[slot, at, :], key_ref[count], preferred_element_type=F32)
            lane = lax.broadcasted_iota(jnp.int32, scores.shape, 1)
            key_at = lane + jnp.where(lane < rows, offset * rows, (7 - offset) * rows - rows)
            row = block + lax.broadcasted_iota(jnp.int32, scores.shape, 0)
            owns = [2 * lax.rem(y + shift + 4, 4) + core for shift in steps]
            owns = [jnp.where(slot == 0, own, 7 - own) for own in owns]
            own = jnp.where(row < 2 * rows, owns[0], owns[-1])
            scores = jnp.where(key_at <= own * rows + row % rows, scores, MASKED)
            score_ref[0, at, :] = scores
            max_ref[at, :] = jnp.broadcast_to(jnp.max(scores, axis=1, keepdims=True), (TALL, 128))
            acc_ref[at, :] = jnp.zeros((TALL, 128), F32)

        def add_slab(slab, held, block):
            at = pl.ds(block, TALL)
            highest = jnp.concatenate([max_ref[at, :]] * 4, axis=1)
            weights = jnp.exp(score_ref[held, at, :] - highest).astype(BF16)
            acc_ref[at, :] += jnp.dot(weights, value_ref[slab], preferred_element_type=F32)

        def next_slab(turn, carry):
            slab = count - turn
            held = lax.rem(turn, 2)
            peaks = []
            for block in blocks:
                at = pl.ds(block, TALL)
                scores = jnp.dot(
                    query_ref[slot, at, :], key_ref[slab - 1], preferred_element_type=F32
                )
                score_ref[1 - held, at, :] = scores
                highest = jnp.concatenate([max_ref[at, :]] * 4, axis=1)
                peaks.append(jnp.max(scores - highest))
                add_slab(slab, held, block)

            @pl.when(functools.reduce(jnp.maximum, peaks) > 60.0)
            def _():
                for block in blocks:
                    at = pl.ds(block, TALL)
                    old = max_ref[at, :]
                    top = jnp.max(score_ref[1 - held, at, :], axis=1, keepdims=True)
                    new = jnp.maximum(old, top)
                    acc_ref[at, :] = acc_ref[at, :] * jnp.exp(old - new)
                    max_ref[at, :] = new

            return carry

        lax.fori_loop(0, count, next_slab, 0)
        for block in blocks:
            add_slab(0, lax.rem(count, 2), block)
        lane = lax.broadcasted_iota(jnp.int32, (2 * rows, 128), 1)
        for number in range(count_y):
            at = pl.ds(number * 2 * rows, 2 * rows)
            total = acc_ref[at, :]
            weight = total[:, HD : HD + 1]
            first, second, third = pieces_of(max_ref[at, :] + jnp.log(weight))
            stats = jnp.where(lane < 80, first, jnp.where(lane < 96, second, third))
            o_refs[number][slot] = jnp.where(lane < HD, total / weight, stats).astype(BF16)
        return carry

    lax.fori_loop(0, 2, run_half, 0)


TALL = 1024


def attention(own, steps, query_parts, keys, values):
    rows = query_parts[0].shape[2]
    count_y = len(steps)
    shape = (2, 2 * rows, 128)
    operands = (*query_parts, keys, values)
    return pl.pallas_call(
        functools.partial(attention_body, steps=steps),
        grid_spec=pltpu.PrefetchScalarGridSpec(
            num_scalar_prefetch=1,
            grid=(1,),
            in_specs=[whole(x.shape) for x in operands],
            out_specs=[whole(shape)] * count_y,
            scratch_shapes=[
                pltpu.VMEM((2, 2 * count_y * rows, HEAD_ROWS), BF16),
                pltpu.VMEM((2 * count_y * rows, 128), F32),
                pltpu.VMEM((2 * count_y * rows, 128), F32),
                pltpu.VMEM((2, 2 * count_y * rows, 2 * rows), F32),
            ],
        ),
        out_shape=[jax.ShapeDtypeStruct(shape, BF16)] * count_y,
        cost_estimate=pl.CostEstimate(
            flops=10_000_000_000, transcendentals=5_000_000, bytes_accessed=2_000_000
        ),
        name="attention",
    )(own, *operands)


def merge_body(a, b, c, d, keep_ref, send_ref):
    rows = keep_ref.shape[0]
    for slot, target in enumerate((keep_ref, send_ref)):
        parts = [ref[slot].astype(F32) for ref in (a, b, c, d)]
        logs = [x[:, 64:65] + x[:, 80:81] + x[:, 96:97] for x in parts]
        highest = functools.reduce(jnp.maximum, logs)
        shares = [jnp.exp(x - highest) for x in logs]
        total = functools.reduce(jnp.add, shares)
        mixed = functools.reduce(jnp.add, [x * share for x, share in zip(parts, shares)]) / total
        target[...] = jnp.concatenate([mixed[:rows, :HD], mixed[rows:, :HD]], axis=1).astype(BF16)


def merge(parts):
    rows = parts[0].shape[1] // 2
    return pl.pallas_call(
        merge_body,
        out_shape=[jax.ShapeDtypeStruct((rows, 128), BF16)] * 2,
        name="merge",
    )(*parts)


def project_body(own_ref, tp_ref, keep_ref, back_ref, w_ref, *out_refs):
    tp = len(out_refs)
    even = lax.rem(own_ref[0], 2) == 0
    rows = out_refs[0].shape[0]
    for shift, ref in enumerate(out_refs):
        at = pl.multiple_of(lax.rem(tp_ref[0] + shift, tp) * rows, rows)
        kept, back = keep_ref[pl.ds(at, rows), :], back_ref[pl.ds(at, rows), :]
        attended = jnp.concatenate(
            [jnp.where(even, kept, back), jnp.where(even, back, kept)], axis=1
        )
        ref[...] = jnp.dot(attended, w_ref[...], preferred_element_type=F32).astype(BF16)


def project(own, tp_index, keep, back, out_weight, tp):
    shape = (keep.shape[0] // tp, out_weight.shape[1])
    return pl.pallas_call(
        project_body,
        grid_spec=pltpu.PrefetchScalarGridSpec(
            num_scalar_prefetch=2,
            grid=(1,),
            in_specs=[whole(x.shape) for x in (keep, back, out_weight)],
            out_specs=[whole(shape)] * tp,
        ),
        out_shape=[jax.ShapeDtypeStruct(shape, BF16)] * tp,
        name="project",
    )(own, tp_index, keep, back, out_weight)


CHUNKS = 1


def slot_number(named, rank, expert_at, cap, chunk, axis):
    part = cap // CHUNKS
    base = (expert_at * part).astype(F32)
    number = base + rank
    for cut in range(1, CHUNKS):
        number = number + jnp.where(rank >= cut * part, float(chunk - part), 0.0)
    return jnp.sum(named * number, axis=axis, keepdims=True).astype(jnp.int32)


def dispatch_body(
    index_ref, rows_ref, part_ref, gain_ref, experts_t_ref, *send_refs, cap
):
    tokens = rows_ref.shape[0]
    chunk = send_refs[0].shape[0]
    slots = chunk * len(send_refs)
    count = slots // cap
    rows = rows_ref[...].astype(F32)
    scale = lax.rsqrt(jnp.mean(rows * rows, axis=1, keepdims=True) + EPSILON)
    normed = (part_ref[...].astype(F32) * scale * gain_ref[...]).astype(BF16)
    expert_at = lax.broadcasted_iota(jnp.int32, (count, tokens), 0)
    first = (expert_at == experts_t_ref[0:1, :]).astype(F32)
    second = (expert_at == experts_t_ref[1:2, :]).astype(F32)
    earlier = (
        lax.broadcasted_iota(jnp.int32, (tokens, tokens), 0)
        < lax.broadcasted_iota(jnp.int32, (tokens, tokens), 1)
    ).astype(BF16)
    before_first = jnp.dot(first.astype(BF16), earlier, preferred_element_type=F32)
    before_second = jnp.dot(second.astype(BF16), earlier, preferred_element_type=F32) + jnp.sum(
        first, axis=1, keepdims=True
    )
    to_first = slot_number(first, before_first, expert_at, cap, chunk, 0)
    to_second = slot_number(second, before_second, expert_at, cap, chunk, 0)
    slot_at = lax.broadcasted_iota(jnp.int32, (slots, tokens), 0)
    chosen = ((slot_at == to_first) | (slot_at == to_second)).astype(F32).astype(BF16)
    for number, ref in enumerate(send_refs):
        picks = chosen[number * chunk : (number + 1) * chunk]
        ref[...] = jnp.dot(picks, normed, preferred_element_type=F32).astype(BF16)


def dispatch(tp_index, moe_rows, norm_gain, experts, count, tp):
    tokens, width = moe_rows.shape
    cap = 4 * tokens // count
    part = width // tp
    return pl.pallas_call(
        functools.partial(dispatch_body, cap=cap),
        grid_spec=pltpu.PrefetchScalarGridSpec(
            num_scalar_prefetch=1,
            grid=(1,),
            in_specs=[
                whole(moe_rows.shape),
                pl.BlockSpec((tokens, part), lambda s, own: (0, own[0])),
                pl.BlockSpec((1, part), lambda s, own: (0, own[0])),
                whole((2, tokens)),
            ],
            out_specs=[whole((count * cap // CHUNKS, part))] * CHUNKS,
        ),
        out_shape=[jax.ShapeDtypeStruct((count * cap // CHUNKS, part), BF16)] * CHUNKS,
        name="dispatch",
    )(tp_index, moe_rows, moe_rows, norm_gain.reshape(1, -1), experts.T)


def way_back_body(experts_ref, slot_ref, *, count, cap):
    tokens = experts_ref.shape[0]
    expert_at = lax.broadcasted_iota(jnp.int32, (tokens, count), 1)
    first = (expert_at == experts_ref[:, 0:1]).astype(F32)
    second = (expert_at == experts_ref[:, 1:2]).astype(F32)
    earlier = (
        lax.broadcasted_iota(jnp.int32, (tokens, tokens), 1)
        < lax.broadcasted_iota(jnp.int32, (tokens, tokens), 0)
    ).astype(BF16)
    before_first = jnp.dot(earlier, first.astype(BF16), preferred_element_type=F32)
    before_second = jnp.dot(earlier, second.astype(BF16), preferred_element_type=F32) + jnp.sum(
        first, axis=0, keepdims=True
    )
    chunk = count * cap // CHUNKS
    slot_ref[:, 0:1] = slot_number(first, before_first, expert_at, cap, chunk, 1)
    slot_ref[:, 1:2] = slot_number(second, before_second, expert_at, cap, chunk, 1)


def way_back(experts, count):
    cap = 4 * experts.shape[0] // count
    return pl.pallas_call(
        functools.partial(way_back_body, count=count, cap=cap),
        out_shape=jax.ShapeDtypeStruct(experts.shape, jnp.int32),
        name="way_back",
    )(experts)


def pick_parts(index_ref, refs, steps):
    own, previous, following, far_low, far_high = refs
    low = pl.program_id(0) < steps // 2
    tp = index_ref[0]
    return (
        (tp, own[...]),
        (lax.rem(tp + 3, 4), previous[...]),
        (lax.rem(tp + 1, 4), following[...]),
        (lax.rem(tp + 2, 4), jnp.where(low, far_low[...], far_high[...])),
    )


def part_specs(tall, wide, steps):
    block = tall // steps
    half = steps // 2
    straight = pl.BlockSpec((block, wide), lambda s, own: (s, 0))
    return [
        straight,
        straight,
        straight,
        pl.BlockSpec((block, wide), lambda s, own: (jnp.minimum(s, half - 1), 0)),
        pl.BlockSpec((block, wide), lambda s, own: (jnp.maximum(s - half, 0), 0)),
    ]


def up_body(index_ref, a, b, c, d, e, gate_ref, up_ref, out_ref, *, steps):
    gate = up = None
    for number, rows in pick_parts(index_ref, (a, b, c, d, e), steps):
        to_gate = jnp.dot(rows, gate_ref[number], preferred_element_type=F32)
        to_up = jnp.dot(rows, up_ref[number], preferred_element_type=F32)
        gate = to_gate if gate is None else gate + to_gate
        up = to_up if up is None else up + to_up
    out_ref[...] = (gate / (1.0 + jnp.exp(-gate)) * up).astype(BF16)


def up_projections(tp_index, parts, w_gate, w_up, tp):
    tall, wide = parts[0].shape
    steps = 4
    hidden = w_gate.shape[1]
    return pl.pallas_call(
        functools.partial(up_body, steps=steps),
        grid_spec=pltpu.PrefetchScalarGridSpec(
            num_scalar_prefetch=1,
            grid=(steps,),
            in_specs=part_specs(tall, wide, steps)
            + [whole((tp, wide, hidden)), whole((tp, wide, hidden))],
            out_specs=pl.BlockSpec((tall // steps, hidden), lambda s, own: (s, 0)),
        ),
        out_shape=jax.ShapeDtypeStruct((tall, hidden), BF16),
        cost_estimate=pl.CostEstimate(
            flops=2_200_000_000, transcendentals=262_144, bytes_accessed=6_800_000
        ),
        name="up_projections",
    )(tp_index, *parts, w_gate.reshape(tp, wide, hidden), w_up.reshape(tp, wide, hidden))


def down_body(index_ref, a, b, c, d, e, own_w, previous_w, following_w, far_w, out_ref, *, steps):
    low = pl.program_id(0) < steps // 2
    far_rows = jnp.where(low, d[...], e[...])
    total = jnp.dot(a[...], own_w[...], preferred_element_type=F32)
    total = total + jnp.dot(b[...], previous_w[...], preferred_element_type=F32)
    total = total + jnp.dot(c[...], following_w[...], preferred_element_type=F32)
    total = total + jnp.dot(far_rows, far_w[...], preferred_element_type=F32)
    out_ref[...] = total.astype(BF16)


def down_projection(tp_index, parts, w_down, moved):
    tall, wide = parts[0].shape
    steps = 4
    columns = moved[0].shape[1]
    return pl.pallas_call(
        functools.partial(down_body, steps=steps),
        grid_spec=pltpu.PrefetchScalarGridSpec(
            num_scalar_prefetch=1,
            grid=(steps,),
            in_specs=part_specs(tall, wide, steps)
            + [pl.BlockSpec((wide, columns), lambda s, own: (0, own[0]))]
            + [whole((wide, columns))] * 3,
            out_specs=pl.BlockSpec((tall // steps, columns), lambda s, own: (s, 0)),
        ),
        out_shape=jax.ShapeDtypeStruct((tall, columns), BF16),
        cost_estimate=pl.CostEstimate(
            flops=1_100_000_000, transcendentals=0, bytes_accessed=4_200_000
        ),
        name="down_projection",
    )(tp_index, *parts, w_down, *moved)


def cut_body(index_ref, a, b, c, to_a, to_b, to_c):
    to_a[...] = a[...]
    to_b[...] = b[...]
    to_c[...] = c[...]


def cut_columns(tp_index, w_down, tp):
    wide, columns = w_down.shape[0], w_down.shape[1] // tp

    def block(shift):
        return pl.BlockSpec((wide, columns), lambda s, own: (0, lax.rem(own[0] + shift, tp)))

    return pl.pallas_call(
        cut_body,
        grid_spec=pltpu.PrefetchScalarGridSpec(
            num_scalar_prefetch=1,
            grid=(1,),
            in_specs=[block(1), block(tp - 1), block(2)],
            out_specs=[whole((wide, columns))] * 3,
        ),
        out_shape=[jax.ShapeDtypeStruct((wide, columns), BF16)] * 3,
        name="cut_columns",
    )(tp_index, w_down, w_down, w_down)


def combine_body(slot_ref, weight_ref, *refs):
    row_refs, out_ref = refs[:-1], refs[-1]
    chunk = row_refs[0].shape[0]
    tokens = slot_ref.shape[0]
    total = None
    for k in range(2):
        picked = None
        for number, ref in enumerate(row_refs):
            slot_at = number * chunk + lax.broadcasted_iota(jnp.int32, (tokens, chunk), 1)
            chosen = (slot_at == slot_ref[:, k : k + 1]).astype(F32).astype(BF16)
            found = jnp.dot(chosen, ref[...], preferred_element_type=F32)
            picked = found if picked is None else picked + found
        term = picked * weight_ref[:, k : k + 1]
        total = term if total is None else total + term
    out_ref[...] = total.astype(BF16)


def combine(slots, expert_weights, rows):
    return pl.pallas_call(
        combine_body,
        out_shape=jax.ShapeDtypeStruct((slots.shape[0], rows[0].shape[1]), BF16),
        name="combine",
    )(slots, expert_weights, *rows)


def per_device(
    queries,
    keys,
    values,
    log_gates,
    out_weight,
    moe_rows,
    norm_gain,
    experts,
    expert_weights,
    w_gate,
    w_up,
    w_down,
):
    size = lax.axis_size("ep")
    tp = lax.axis_size("tp")
    own = lax.axis_index("ep").astype(jnp.int32).reshape(1)
    tp_index = lax.axis_index("tp").astype(jnp.int32).reshape(1)
    up_ring = [(n, (n + 1) % tp) for n in range(tp)]
    down_ring = [(n, (n - 1) % tp) for n in range(tp)]

    def over_ep(x):
        wide = x.shape[1]
        moved = lax.all_to_all(
            x.reshape(size, -1, wide), "ep", split_axis=0, concat_axis=0, tiled=True
        )
        return moved.reshape(-1, wide)

    def near(x):
        return lax.ppermute(x, "tp", up_ring), lax.ppermute(x, "tp", down_ring)

    def far(pair):
        half = pair[0].shape[0] // 2
        low, high = pair[0][:half], pair[1][half:]
        return lax.ppermute(low, "tp", up_ring), lax.ppermute(high, "tp", down_ring)

    keep, send = pack(own, queries, keys, values, log_gates.T)
    mirrored = lax.ppermute(send, "ep", mirror_pairs(size))
    outgoing = dispatch(tp_index, moe_rows, norm_gain, experts, size, tp)
    arrived = []
    for rows in outgoing:
        arrived.append(over_ep(rows))
    both = jnp.stack([keep, mirrored])
    own_keys, own_queries = both[:, :KV_ROWS], both[:, KV_ROWS:]
    query_parts = [own_queries] + [
        lax.ppermute(own_queries, "ep", along_y(-step, size)) for step in Y_STEPS[1:]
    ]
    below2, above2, below, above = [
        lax.ppermute(own_keys, "ep", along_z(shift, size)) for shift in (2, -2, 1, -1)
    ]
    below3 = lax.ppermute(below2, "ep", along_z(1, size))
    above3 = lax.ppermute(above2, "ep", along_z(-1, size))
    far_low = lax.ppermute(below2[:1], "ep", along_z(2, size))
    far_high = lax.ppermute(above2[1:], "ep", along_z(-2, size))
    kv_parts = [own_keys, below, above, below2, above2, below3, above3, far_low, far_high]
    slab_keys, slab_values = assemble(own, kv_parts)
    far_ring = [(n, (n + 2) % tp) for n in range(tp)]
    cuts = cut_columns(tp_index, w_down[0], tp)
    moved = [
        lax.ppermute(cut, "tp", ring) for cut, ring in zip(cuts, (up_ring, down_ring, far_ring))
    ]
    slots = way_back(experts, size)
    x_near = [near(rows) for rows in arrived]
    x_far = [far(pair) for pair in x_near]
    partial = {}
    for picks in ((3, 1), (2, 0)):
        done = attention(
            own,
            tuple(Y_STEPS[n] for n in picks),
            [query_parts[n] for n in picks],
            slab_keys,
            slab_values,
        )
        for n, part in zip(picks, done):
            if n:
                part = lax.ppermute(part, "ep", along_y(Y_STEPS[n], size))
            partial[n] = part
    h_near, h_far, hidden = [], [], []
    for number in range(CHUNKS):
        hidden.append(
            up_projections(
                tp_index,
                (arrived[number],) + x_near[number] + x_far[number],
                w_gate[0],
                w_up[0],
                tp,
            )
        )
        h_near.append(near(hidden[number]))
        h_far.append(far(h_near[number]))
    kept, sent = merge([partial[n] for n in range(4)])
    back = lax.ppermute(sent, "ep", mirror_pairs(size))
    products = project(own, tp_index, kept, back, out_weight, tp)
    others = [
        lax.ppermute(product, "tp", ring)
        for product, ring in zip(products[1:], (up_ring, far_ring, down_ring))
    ]
    mixed = sum(part.astype(F32) for part in [products[0]] + others).astype(BF16)
    returned = []
    for number in range(CHUNKS):
        result = down_projection(
            tp_index, (hidden[number],) + h_near[number] + h_far[number], w_down[0], moved
        )
        returned.append(over_ep(result))
    moe_out = combine(slots, expert_weights, returned)
    return (mixed, moe_out)


def solution(mesh):
    placed = (
        P("ep", "tp"),
        P("ep", "tp"),
        P("ep", "tp"),
        P("ep", "tp"),
        P("tp", None),
        P("ep", None),
        P(),
        P("ep", None),
        P("ep", None),
        P("ep", None, "tp"),
        P("ep", None, "tp"),
        P("ep", "tp", None),
    )
    return jax.shard_map(
        per_device,
        mesh=mesh,
        in_specs=placed,
        out_specs=(P(("ep", "tp"), None), P("ep", "tp")),
        check_vma=False,
    )
```

```python
import functools

import jax
import jax.numpy as jnp
from jax import lax
from jax.experimental import pallas as pl
from jax.experimental.pallas import tpu as pltpu
from jax.sharding import PartitionSpec as P


HD = 64
EPSILON = 1e-06
MASKED = -1e30
F32 = jnp.float32
BF16 = jnp.bfloat16
HEAD_ROWS = 80


def whole(shape):
    return pl.BlockSpec(shape, lambda *_: (0,) * len(shape))


def mirror_pairs(size):
    return [(n, size - 1 - n) for n in range(size)]


def along_z(shift, size):
    return [(n, (n + 8 * shift) % size) for n in range(size)]


def along_y(shift, size):
    return [(n, n // 8 * 8 + (n // 2 + shift) % 4 * 2 + n % 2) for n in range(size)]


Y_STEPS = (0, -1, 1, 2)
Z_STEPS = (0, -1, 1, -2, 2, -3, 3)
KV_ROWS = HEAD_ROWS + HD


def pieces_of(value):
    high = value.astype(BF16).astype(F32)
    rest = value - high
    mid = rest.astype(BF16).astype(F32)
    return high, mid, rest - mid


def pack_body(own_ref, queries_ref, keys_ref, values_ref, gates_ref, keep_ref, send_ref):
    rows = keys_ref.shape[0]
    half = rows // 2
    keys_t = keys_ref[...].astype(F32).T
    values_t = values_ref[...].astype(F32).T
    split = pieces_of(gates_ref[...])
    pad = jnp.zeros((HEAD_ROWS - HD - 6, rows), F32)
    blocks = []
    for g in range(2):
        gates = [piece[2 * g + r : 2 * g + r + 1] for r in range(2) for piece in split]
        heads = slice(g * HD, (g + 1) * HD)
        upper = jnp.concatenate([keys_t[heads]] + gates + [pad, values_t[heads]], axis=0)
        wide = queries_ref[:, g * 128 : (g + 1) * 128].astype(F32)
        lower = jnp.concatenate([wide[:half], wide[half:]], axis=1)
        blocks.append(jnp.concatenate([upper, lower], axis=0).astype(BF16))
    even = lax.rem(own_ref[0], 2) == 0

    @pl.when(even)
    def _():
        keep_ref[...] = blocks[0]
        send_ref[...] = blocks[1]

    @pl.when(jnp.logical_not(even))
    def _():
        keep_ref[...] = blocks[1]
        send_ref[...] = blocks[0]


def pack(own, queries, keys, values, gates_t):
    rows = keys.shape[0]
    shape = (KV_ROWS + rows // 2, rows)
    return pl.pallas_call(
        pack_body,
        grid_spec=pltpu.PrefetchScalarGridSpec(
            num_scalar_prefetch=1,
            grid=(1,),
            in_specs=[whole(x.shape) for x in (queries, keys, values, gates_t)],
            out_specs=[whole(shape), whole(shape)],
        ),
        out_shape=[jax.ShapeDtypeStruct(shape, BF16)] * 2,
        name="pack",
    )(own, queries, keys, values, gates_t)


def assemble_body(own_ref, *refs):
    kv_refs, key_ref, value_ref = refs[:9], refs[9], refs[10]
    z = own_ref[0] // 8
    rows = kv_refs[0].shape[2]
    ones = jnp.ones((rows, HD), F32)

    def place_keys(slab, at, block):
        key_ref[slab, :, pl.ds(at * rows, rows)] = block[:HEAD_ROWS]
        turned = block[HEAD_ROWS:].astype(F32).T
        value_ref[slab, pl.ds(at * rows, rows), :] = jnp.concatenate(
            [turned, ones], axis=1
        ).astype(BF16)

    for number, shift in enumerate(Z_STEPS):
        source = lax.rem(z + shift + 8, 8)
        place_keys(source, 0, kv_refs[number][0])
        place_keys(7 - source, 1, kv_refs[number][1])
    source = lax.rem(z + 4, 8)
    place_keys(source, 0, kv_refs[7][0])
    place_keys(7 - source, 1, kv_refs[8][0])


def assemble(own, kv_parts):
    rows = kv_parts[0].shape[2]
    shapes = [(8, HEAD_ROWS, 2 * rows), (8, 2 * rows, 128)]
    return pl.pallas_call(
        assemble_body,
        grid_spec=pltpu.PrefetchScalarGridSpec(
            num_scalar_prefetch=1,
            grid=(1,),
            in_specs=[whole(x.shape) for x in kv_parts],
            out_specs=[whole(shape) for shape in shapes],
        ),
        out_shape=[jax.ShapeDtypeStruct(shape, BF16) for shape in shapes],
        name="assemble",
    )(own, *kv_parts)


def attention_body(own_ref, *refs, steps):
    count_y = len(steps)
    q_refs, (key_ref, value_ref) = refs[:count_y], refs[count_y : count_y + 2]
    o_refs = refs[count_y + 2 : 2 * count_y + 2]
    query_ref, acc_ref, max_ref, score_ref = refs[2 * count_y + 2 :]
    z, y, core = own_ref[0] // 8, own_ref[0] // 2 % 4, own_ref[0] % 2
    rows = q_refs[0].shape[2]
    column = lax.broadcasted_iota(jnp.int32, (rows, HEAD_ROWS - HD), 1)
    for number, ref in enumerate(q_refs):
        for slot in range(2):
            packed = ref[slot].astype(F32) * HD ** (-0.5)
            both = jnp.concatenate([packed[:, :128], packed[:, 128:]], axis=0)
            for r in range(2):
                picks = jnp.where((column >= 3 * r) & (column < 3 * r + 3), -1.0, 0.0)
                query_ref[slot, pl.ds((2 * number + r) * rows, rows), :] = jnp.concatenate(
                    [both[:, r * HD : (r + 1) * HD], picks.astype(F32)], axis=1
                ).astype(BF16)
    low = jnp.minimum(z, 7 - z)
    offset = 2 * y + core

    blocks = range(0, 2 * count_y * rows, TALL)

    def run_half(high, carry):
        count = jnp.where(high == 1, 7 - low, low)
        slot = jnp.where(count == z, 0, 1)
        owns = [2 * lax.rem(y + shift + 4, 4) + core for shift in steps]
        owns = [jnp.where(slot == 0, own, 7 - own) for own in owns]

        def own_slab(block, carry):
            at = pl.ds(pl.multiple_of(block * 2 * rows, 2 * rows), 2 * rows)
            scores = jnp.dot(query_ref[slot, at, :], key_ref[count], preferred_element_type=F32)
            lane = lax.broadcasted_iota(jnp.int32, scores.shape, 1)
            key_at = lane + jnp.where(lane < rows, offset * rows, (7 - offset) * rows - rows)
            own = owns[0]
            for number in range(1, count_y):
                own = jnp.where(block < number, own, owns[number])
            row = lax.broadcasted_iota(jnp.int32, scores.shape, 0)
            query_at = own * rows + jnp.where(row < rows, row, row - rows)
            scores = jnp.where(key_at <= query_at, scores, MASKED)
            score_ref[0, at, :] = scores
            top = jnp.max(scores, axis=1, keepdims=True)
            max_ref[at, :] = jnp.broadcast_to(top, (2 * rows, 128))
            acc_ref[at, :] = jnp.zeros((2 * rows, 128), F32)
            return carry

        lax.fori_loop(0, count_y, own_slab, 0)

        def add_slab(slab, held, block):
            at = pl.ds(block, TALL)
            highest = jnp.concatenate([max_ref[at, :]] * 4, axis=1)
            weights = jnp.exp(score_ref[held, at, :] - highest).astype(BF16)
            acc_ref[at, :] += jnp.dot(weights, value_ref[slab], preferred_element_type=F32)

        def next_slab(turn, carry):
            slab = count - turn
            held = lax.rem(turn, 2)
            peaks = []
            for block in blocks:
                at = pl.ds(block, TALL)
                scores = jnp.dot(
                    query_ref[slot, at, :], key_ref[slab - 1], preferred_element_type=F32
                )
                score_ref[1 - held, at, :] = scores
                highest = jnp.concatenate([max_ref[at, :]] * 4, axis=1)
                peaks.append(jnp.max(scores - highest))
                add_slab(slab, held, block)

            @pl.when(functools.reduce(jnp.maximum, peaks) > 60.0)
            def _():
                def raise_rows(block, carry):
                    at = pl.ds(pl.multiple_of(block * rows, rows), rows)
                    old = max_ref[at, :]
                    top = jnp.max(score_ref[1 - held, at, :], axis=1, keepdims=True)
                    new = jnp.maximum(old, top)
                    acc_ref[at, :] = acc_ref[at, :] * jnp.exp(old - new)
                    max_ref[at, :] = new
                    return carry

                lax.fori_loop(0, 2 * count_y, raise_rows, 0)

            return carry

        lax.fori_loop(0, count, next_slab, 0)
        for block in blocks:
            add_slab(0, lax.rem(count, 2), block)
        lane = lax.broadcasted_iota(jnp.int32, (2 * rows, 128), 1)
        for number in range(count_y):
            at = pl.ds(number * 2 * rows, 2 * rows)
            total = acc_ref[at, :]
            weight = total[:, HD : HD + 1]
            first, second, third = pieces_of(max_ref[at, :] + jnp.log(weight))
            stats = jnp.where(lane < 80, first, jnp.where(lane < 96, second, third))
            o_refs[number][slot] = jnp.where(lane < HD, total / weight, stats).astype(BF16)
        return carry

    lax.fori_loop(0, 2, run_half, 0)


TALL = 1024


def attention(own, steps, query_parts, keys, values):
    rows = query_parts[0].shape[2]
    count_y = len(steps)
    shape = (2, 2 * rows, 128)
    operands = (*query_parts, keys, values)
    return pl.pallas_call(
        functools.partial(attention_body, steps=steps),
        grid_spec=pltpu.PrefetchScalarGridSpec(
            num_scalar_prefetch=1,
            grid=(1,),
            in_specs=[whole(x.shape) for x in operands],
            out_specs=[whole(shape)] * count_y,
            scratch_shapes=[
                pltpu.VMEM((2, 2 * count_y * rows, HEAD_ROWS), BF16),
                pltpu.VMEM((2 * count_y * rows, 128), F32),
                pltpu.VMEM((2 * count_y * rows, 128), F32),
                pltpu.VMEM((2, 2 * count_y * rows, 2 * rows), F32),
            ],
        ),
        out_shape=[jax.ShapeDtypeStruct(shape, BF16)] * count_y,
        cost_estimate=pl.CostEstimate(
            flops=10_000_000_000, transcendentals=5_000_000, bytes_accessed=2_000_000
        ),
        name="attention",
    )(own, *operands)


def merge_body(a, b, c, d, keep_ref, send_ref):
    rows = keep_ref.shape[0]
    for slot, target in enumerate((keep_ref, send_ref)):
        parts = [ref[slot].astype(F32) for ref in (a, b, c, d)]
        logs = [x[:, 64:65] + x[:, 80:81] + x[:, 96:97] for x in parts]
        highest = functools.reduce(jnp.maximum, logs)
        shares = [jnp.exp(x - highest) for x in logs]
        total = functools.reduce(jnp.add, shares)
        mixed = functools.reduce(jnp.add, [x * share for x, share in zip(parts, shares)]) / total
        target[...] = jnp.concatenate([mixed[:rows, :HD], mixed[rows:, :HD]], axis=1).astype(BF16)


def merge(parts):
    rows = parts[0].shape[1] // 2
    return pl.pallas_call(
        merge_body,
        out_shape=[jax.ShapeDtypeStruct((rows, 128), BF16)] * 2,
        name="merge",
    )(*parts)


def project_body(own_ref, tp_ref, keep_ref, back_ref, w_ref, *out_refs):
    tp = len(out_refs)
    even = lax.rem(own_ref[0], 2) == 0
    rows = out_refs[0].shape[0]
    for shift, ref in enumerate(out_refs):
        at = pl.multiple_of(lax.rem(tp_ref[0] + shift, tp) * rows, rows)
        kept, back = keep_ref[pl.ds(at, rows), :], back_ref[pl.ds(at, rows), :]
        attended = jnp.concatenate(
            [jnp.where(even, kept, back), jnp.where(even, back, kept)], axis=1
        )
        ref[...] = jnp.dot(attended, w_ref[...], preferred_element_type=F32).astype(BF16)


def project(own, tp_index, keep, back, out_weight, tp):
    shape = (keep.shape[0] // tp, out_weight.shape[1])
    return pl.pallas_call(
        project_body,
        grid_spec=pltpu.PrefetchScalarGridSpec(
            num_scalar_prefetch=2,
            grid=(1,),
            in_specs=[whole(x.shape) for x in (keep, back, out_weight)],
            out_specs=[whole(shape)] * tp,
        ),
        out_shape=[jax.ShapeDtypeStruct(shape, BF16)] * tp,
        name="project",
    )(own, tp_index, keep, back, out_weight)


CHUNKS = 1


def slot_number(named, rank, expert_at, cap, chunk, axis):
    part = cap // CHUNKS
    base = (expert_at * part).astype(F32)
    number = base + rank
    for cut in range(1, CHUNKS):
        number = number + jnp.where(rank >= cut * part, float(chunk - part), 0.0)
    return jnp.sum(named * number, axis=axis, keepdims=True).astype(jnp.int32)


def dispatch_body(
    index_ref, rows_ref, part_ref, gain_ref, experts_t_ref, *send_refs, cap
):
    tokens = rows_ref.shape[0]
    chunk = send_refs[0].shape[0]
    slots = chunk * len(send_refs)
    count = slots // cap
    rows = rows_ref[...].astype(F32)
    scale = lax.rsqrt(jnp.mean(rows * rows, axis=1, keepdims=True) + EPSILON)
    normed = (part_ref[...].astype(F32) * scale * gain_ref[...]).astype(BF16)
    expert_at = lax.broadcasted_iota(jnp.int32, (count, tokens), 0)
    first = (expert_at == experts_t_ref[0:1, :]).astype(F32)
    second = (expert_at == experts_t_ref[1:2, :]).astype(F32)
    earlier = (
        lax.broadcasted_iota(jnp.int32, (tokens, tokens), 0)
        < lax.broadcasted_iota(jnp.int32, (tokens, tokens), 1)
    ).astype(BF16)
    before_first = jnp.dot(first.astype(BF16), earlier, preferred_element_type=F32)
    before_second = jnp.dot(second.astype(BF16), earlier, preferred_element_type=F32) + jnp.sum(
        first, axis=1, keepdims=True
    )
    to_first = slot_number(first, before_first, expert_at, cap, chunk, 0)
    to_second = slot_number(second, before_second, expert_at, cap, chunk, 0)
    slot_at = lax.broadcasted_iota(jnp.int32, (slots, tokens), 0)
    chosen = ((slot_at == to_first) | (slot_at == to_second)).astype(F32).astype(BF16)
    for number, ref in enumerate(send_refs):
        picks = chosen[number * chunk : (number + 1) * chunk]
        ref[...] = jnp.dot(picks, normed, preferred_element_type=F32).astype(BF16)


def dispatch(tp_index, moe_rows, norm_gain, experts, count, tp):
    tokens, width = moe_rows.shape
    cap = 4 * tokens // count
    part = width // tp
    return pl.pallas_call(
        functools.partial(dispatch_body, cap=cap),
        grid_spec=pltpu.PrefetchScalarGridSpec(
            num_scalar_prefetch=1,
            grid=(1,),
            in_specs=[
                whole(moe_rows.shape),
                pl.BlockSpec((tokens, part), lambda s, own: (0, own[0])),
                pl.BlockSpec((1, part), lambda s, own: (0, own[0])),
                whole((2, tokens)),
            ],
            out_specs=[whole((count * cap // CHUNKS, part))] * CHUNKS,
        ),
        out_shape=[jax.ShapeDtypeStruct((count * cap // CHUNKS, part), BF16)] * CHUNKS,
        name="dispatch",
    )(tp_index, moe_rows, moe_rows, norm_gain.reshape(1, -1), experts.T)


def way_back_body(experts_ref, slot_ref, *, count, cap):
    tokens = experts_ref.shape[0]
    expert_at = lax.broadcasted_iota(jnp.int32, (tokens, count), 1)
    first = (expert_at == experts_ref[:, 0:1]).astype(F32)
    second = (expert_at == experts_ref[:, 1:2]).astype(F32)
    earlier = (
        lax.broadcasted_iota(jnp.int32, (tokens, tokens), 1)
        < lax.broadcasted_iota(jnp.int32, (tokens, tokens), 0)
    ).astype(BF16)
    before_first = jnp.dot(earlier, first.astype(BF16), preferred_element_type=F32)
    before_second = jnp.dot(earlier, second.astype(BF16), preferred_element_type=F32) + jnp.sum(
        first, axis=0, keepdims=True
    )
    chunk = count * cap // CHUNKS
    slot_ref[:, 0:1] = slot_number(first, before_first, expert_at, cap, chunk, 1)
    slot_ref[:, 1:2] = slot_number(second, before_second, expert_at, cap, chunk, 1)


def way_back(experts, count):
    cap = 4 * experts.shape[0] // count
    return pl.pallas_call(
        functools.partial(way_back_body, count=count, cap=cap),
        out_shape=jax.ShapeDtypeStruct(experts.shape, jnp.int32),
        name="way_back",
    )(experts)


def part_specs(tall, wide, steps):
    block = tall // steps
    half = steps // 2
    straight = pl.BlockSpec((block, wide), lambda s, own: (s, 0))
    return [
        straight,
        straight,
        straight,
        pl.BlockSpec((block, wide), lambda s, own: (jnp.minimum(s, half - 1), 0)),
        pl.BlockSpec((block, wide), lambda s, own: (jnp.maximum(s - half, 0), 0)),
    ]


def up_body(index_ref, own_ref, *refs, steps):
    halves, (gate_ref, up_ref, out_ref) = refs[:6], refs[6:]
    low = pl.program_id(0) < steps // 2
    parts = [(index_ref[0], own_ref[...])]
    for number, shift in enumerate((3, 1, 2)):
        rows = jnp.where(low, halves[2 * number][...], halves[2 * number + 1][...])
        parts.append((lax.rem(index_ref[0] + shift, 4), rows))
    gate = up = None
    for number, rows in parts:
        to_gate = jnp.dot(rows, gate_ref[number], preferred_element_type=F32)
        to_up = jnp.dot(rows, up_ref[number], preferred_element_type=F32)
        gate = to_gate if gate is None else gate + to_gate
        up = to_up if up is None else up + to_up
    out_ref[...] = (gate / (1.0 + jnp.exp(-gate)) * up).astype(BF16)


def up_projections(tp_index, parts, w_gate, w_up, tp):
    tall, wide = parts[0].shape
    steps = 4
    hidden = w_gate.shape[1]
    return pl.pallas_call(
        functools.partial(up_body, steps=steps),
        grid_spec=pltpu.PrefetchScalarGridSpec(
            num_scalar_prefetch=1,
            grid=(steps,),
            in_specs=part_specs(tall, wide, steps)[:1]
            + part_specs(tall, wide, steps)[3:] * 3
            + [whole((tp, wide, hidden)), whole((tp, wide, hidden))],
            out_specs=pl.BlockSpec((tall // steps, hidden), lambda s, own: (s, 0)),
        ),
        out_shape=jax.ShapeDtypeStruct((tall, hidden), BF16),
        cost_estimate=pl.CostEstimate(
            flops=2_200_000_000, transcendentals=262_144, bytes_accessed=6_800_000
        ),
        name="up_projections",
    )(tp_index, *parts, w_gate.reshape(tp, wide, hidden), w_up.reshape(tp, wide, hidden))


def down_body(index_ref, a, b, c, d, e, own_w, previous_w, following_w, far_w, out_ref, *, steps):
    low = pl.program_id(0) < steps // 2
    far_rows = jnp.where(low, d[...], e[...])
    total = jnp.dot(a[...], own_w[...], preferred_element_type=F32)
    total = total + jnp.dot(b[...], previous_w[...], preferred_element_type=F32)
    total = total + jnp.dot(c[...], following_w[...], preferred_element_type=F32)
    total = total + jnp.dot(far_rows, far_w[...], preferred_element_type=F32)
    out_ref[...] = total.astype(BF16)


def down_projection(tp_index, parts, w_down, moved):
    tall, wide = parts[0].shape
    steps = 4
    columns = moved[0].shape[1]
    return pl.pallas_call(
        functools.partial(down_body, steps=steps),
        grid_spec=pltpu.PrefetchScalarGridSpec(
            num_scalar_prefetch=1,
            grid=(steps,),
            in_specs=part_specs(tall, wide, steps)
            + [pl.BlockSpec((wide, columns), lambda s, own: (0, own[0]))]
            + [whole((wide, columns))] * 3,
            out_specs=pl.BlockSpec((tall // steps, columns), lambda s, own: (s, 0)),
        ),
        out_shape=jax.ShapeDtypeStruct((tall, columns), BF16),
        cost_estimate=pl.CostEstimate(
            flops=1_100_000_000, transcendentals=0, bytes_accessed=4_200_000
        ),
        name="down_projection",
    )(tp_index, *parts, w_down, *moved)


def cut_body(index_ref, a, b, c, to_a, to_b, to_c):
    to_a[...] = a[...]
    to_b[...] = b[...]
    to_c[...] = c[...]


def cut_columns(tp_index, w_down, tp):
    wide, columns = w_down.shape[0], w_down.shape[1] // tp

    def block(shift):
        return pl.BlockSpec((wide, columns), lambda s, own: (0, lax.rem(own[0] + shift, tp)))

    return pl.pallas_call(
        cut_body,
        grid_spec=pltpu.PrefetchScalarGridSpec(
            num_scalar_prefetch=1,
            grid=(1,),
            in_specs=[block(1), block(tp - 1), block(2)],
            out_specs=[whole((wide, columns))] * 3,
        ),
        out_shape=[jax.ShapeDtypeStruct((wide, columns), BF16)] * 3,
        name="cut_columns",
    )(tp_index, w_down, w_down, w_down)


def combine_body(slot_ref, weight_ref, *refs):
    row_refs, out_ref = refs[:-1], refs[-1]
    chunk = row_refs[0].shape[0]
    tokens = slot_ref.shape[0]
    total = None
    for k in range(2):
        picked = None
        for number, ref in enumerate(row_refs):
            slot_at = number * chunk + lax.broadcasted_iota(jnp.int32, (tokens, chunk), 1)
            chosen = (slot_at == slot_ref[:, k : k + 1]).astype(F32).astype(BF16)
            found = jnp.dot(chosen, ref[...], preferred_element_type=F32)
            picked = found if picked is None else picked + found
        term = picked * weight_ref[:, k : k + 1]
        total = term if total is None else total + term
    out_ref[...] = total.astype(BF16)


def combine(slots, expert_weights, rows):
    return pl.pallas_call(
        combine_body,
        out_shape=jax.ShapeDtypeStruct((slots.shape[0], rows[0].shape[1]), BF16),
        name="combine",
    )(slots, expert_weights, *rows)


def per_device(
    queries,
    keys,
    values,
    log_gates,
    out_weight,
    moe_rows,
    norm_gain,
    experts,
    expert_weights,
    w_gate,
    w_up,
    w_down,
):
    size = lax.axis_size("ep")
    tp = lax.axis_size("tp")
    own = lax.axis_index("ep").astype(jnp.int32).reshape(1)
    tp_index = lax.axis_index("tp").astype(jnp.int32).reshape(1)
    up_ring = [(n, (n + 1) % tp) for n in range(tp)]
    down_ring = [(n, (n - 1) % tp) for n in range(tp)]

    def over_ep(x):
        wide = x.shape[1]
        moved = lax.all_to_all(
            x.reshape(size, -1, wide), "ep", split_axis=0, concat_axis=0, tiled=True
        )
        return moved.reshape(-1, wide)

    def near(x):
        return lax.ppermute(x, "tp", up_ring), lax.ppermute(x, "tp", down_ring)

    def far(pair):
        half = pair[0].shape[0] // 2
        low, high = pair[0][:half], pair[1][half:]
        return lax.ppermute(low, "tp", up_ring), lax.ppermute(high, "tp", down_ring)

    keep, send = pack(own, queries, keys, values, log_gates.T)
    mirrored = lax.ppermute(send, "ep", mirror_pairs(size))
    outgoing = dispatch(tp_index, moe_rows, norm_gain, experts, size, tp)
    arrived = []
    for rows in outgoing:
        arrived.append(over_ep(rows))
    both = jnp.stack([keep, mirrored])
    own_keys, own_queries = both[:, :KV_ROWS], both[:, KV_ROWS:]
    query_parts = [own_queries] + [
        lax.ppermute(own_queries, "ep", along_y(-step, size)) for step in Y_STEPS[1:]
    ]
    below2, above2, below, above = [
        lax.ppermute(own_keys, "ep", along_z(shift, size)) for shift in (2, -2, 1, -1)
    ]
    below3 = lax.ppermute(below2, "ep", along_z(1, size))
    above3 = lax.ppermute(above2, "ep", along_z(-1, size))
    far_low = lax.ppermute(below2[:1], "ep", along_z(2, size))
    far_high = lax.ppermute(above2[1:], "ep", along_z(-2, size))
    kv_parts = [own_keys, below, above, below2, above2, below3, above3, far_low, far_high]
    slab_keys, slab_values = assemble(own, kv_parts)
    far_ring = [(n, (n + 2) % tp) for n in range(tp)]
    cuts = cut_columns(tp_index, w_down[0], tp)
    moved = [
        lax.ppermute(cut, "tp", ring) for cut, ring in zip(cuts, (up_ring, down_ring, far_ring))
    ]
    slots = way_back(experts, size)
    x_parts = []
    for rows in arrived:
        half = rows.shape[0] // 2
        low, high = lax.optimization_barrier((rows[:half], rows[half:]))
        previous_low = lax.ppermute(low, "tp", up_ring)
        following_high = lax.ppermute(high, "tp", down_ring)
        previous_high = lax.ppermute(high, "tp", up_ring)
        following_low = lax.ppermute(low, "tp", down_ring)
        far_low = lax.ppermute(previous_low, "tp", up_ring)
        far_high = lax.ppermute(following_high, "tp", down_ring)
        x_parts.append(
            (rows, previous_low, previous_high, following_low, following_high, far_low, far_high)
        )
    partial = {}
    for picks in ((3, 1), (2, 0)):
        done = attention(
            own,
            tuple(Y_STEPS[n] for n in picks),
            [query_parts[n] for n in picks],
            slab_keys,
            slab_values,
        )
        for n, part in zip(picks, done):
            if n:
                part = lax.ppermute(part, "ep", along_y(Y_STEPS[n], size))
            partial[n] = part
    h_near, h_far, hidden = [], [], []
    for number in range(CHUNKS):
        hidden.append(
            up_projections(
                tp_index,
                x_parts[number],
                w_gate[0],
                w_up[0],
                tp,
            )
        )
        h_near.append(near(hidden[number]))
        h_far.append(far(h_near[number]))
    kept, sent = merge([partial[n] for n in range(4)])
    back = lax.ppermute(sent, "ep", mirror_pairs(size))
    products = project(own, tp_index, kept, back, out_weight, tp)
    others = [
        lax.ppermute(product, "tp", ring)
        for product, ring in zip(products[1:], (up_ring, far_ring, down_ring))
    ]
    mixed = sum(part.astype(F32) for part in [products[0]] + others).astype(BF16)
    returned = []
    for number in range(CHUNKS):
        result = down_projection(
            tp_index, (hidden[number],) + h_near[number] + h_far[number], w_down[0], moved
        )
        returned.append(over_ep(result))
    moe_out = combine(slots, expert_weights, returned)
    return (mixed, moe_out)


def solution(mesh):
    placed = (
        P("ep", "tp"),
        P("ep", "tp"),
        P("ep", "tp"),
        P("ep", "tp"),
        P("tp", None),
        P("ep", None),
        P(),
        P("ep", None),
        P("ep", None),
        P("ep", None, "tp"),
        P("ep", None, "tp"),
        P("ep", "tp", None),
    )
    return jax.shard_map(
        per_device,
        mesh=mesh,
        in_specs=placed,
        out_specs=(P(("ep", "tp"), None), P("ep", "tp")),
        check_vma=False,
    )
```
